128 devices in a mesh: sp: 16 (over z, y), dp: 8 (over x, core).
Axes of the slice: x: 4, y: 4, z: 4, core: 2. Of those that a mesh axis runs over, the one named last changes fastest.
Arguments:
- hidden_in: bfloat16 [8, 2048, 2048], P('dp', 'sp'), may hold values from -6 to 6
- queries: bfloat16 [8, 2048, 1536], P('dp', 'sp'), may hold values from -64 to 64
- key_value_latent: bfloat16 [8, 2048, 512], P('dp', 'sp'), may hold values from -6 to 6
- keys_rope: bfloat16 [8, 2048, 32], P('dp', 'sp'), may hold values from -4 to 4
- latent_norm_gain: float32 [512], replicated, may hold values from 0.1 to 1.9
- latent_up_weight: bfloat16 [512, 2048], replicated, may hold values from -0.25 to 0.25
- attn_gain: float32 [1024], replicated, may hold values from 0.1 to 1.9
- out_proj: bfloat16 [1024, 2048], replicated, may hold values from -0.1875 to 0.1875
- norm1_gain: float32 [2048], replicated, may hold values from 0.1 to 1.9
- norm1_bias: float32 [2048], replicated, may hold values from -1.5 to 1.5
- expert_ids: int32 [8, 2048, 4], P('dp', 'sp'), may hold values from 0 to 127, all different within a row; in each aligned block of 128 rows (0 to 127, 128 to 255, ..., all dimensions but the last counted through in order) at most 6 rows name the same one
- route_weights: float32 [8, 2048, 4], P('dp', 'sp'), may hold values from 0.1 to 1
- gate_proj: bfloat16 [128, 2048, 512], P(('sp', 'dp')), may hold values from -0.125 to 0.125
- up_proj: bfloat16 [128, 2048, 512], P(('sp', 'dp')), may hold values from -0.125 to 0.125
- down_proj: bfloat16 [128, 512, 2048], P(('sp', 'dp')), may hold values from -0.25 to 0.25
- shared_gate: bfloat16 [2048, 512], replicated, may hold values from -0.125 to 0.125
- shared_up: bfloat16 [2048, 512], replicated, may hold values from -0.125 to 0.125
- shared_down: bfloat16 [512, 2048], replicated, may hold values from -0.25 to 0.25
- norm2_gain: float32 [2048], replicated, may hold values from 0.1 to 1.9
- norm2_bias: float32 [2048], replicated, may hold values from -1.5 to 1.5
Outputs:
- result: bfloat16 [8, 2048, 2048], P('dp', 'sp')
The draws below stay inside these ranges and needn't reach their ends.
Inputs may be any that keep to these rules, and one draw needn't show every extreme that they name: `expert_ids`: each row names 4 different experts. Among the rows of one device (aligned blocks of 128 rows), no expert is named more than 6 times, a bound that some block reaches.
All inputs are finite; a program needn't handle non-finite values.
Results may differ from the reference program's by a relative error of at most 0.01.
Values may be sent and summed in bfloat16 or wider, within the bound.
A program may use at most 128 MiB of HBM per device.

```python
import math
import jax
import jax.numpy as jnp
import numpy as np
from jax import lax

D = 2048
ATTENTION_HEADS = 16
PLAIN_HEAD_WIDTH = 64
QK_ROPE = 32
VALUE_HEAD_WIDTH = 64
LATENT_WIDTH = 512
D_EXPERT = 512
D_SHARED = 512
TOP_K = 4
TOK_DEV = 128
SEQUENCE_LENGTH = 2048
BATCH_SEQUENCES = 8
D_ATTN = 1024
EXPERTS = 128
CAP = 6


def rope_base(key):
    inner = jax.random.fold_in(key, 71)
    return jnp.clip(jax.random.normal(inner, (BATCH_SEQUENCES, SEQUENCE_LENGTH, QK_ROPE), jnp.float32), -4.0, 4.0)


def draw_keys_rope(key, part):
    return rope_base(key).astype(jnp.bfloat16)


def draw_queries(key, part):
    head_width = PLAIN_HEAD_WIDTH + QK_ROPE
    inner = jax.random.fold_in(key, 13)
    base = jnp.clip(jax.random.normal(inner, (BATCH_SEQUENCES, SEQUENCE_LENGTH, ATTENTION_HEADS, head_width), jnp.float32), -6.0, 6.0)
    return base.reshape(BATCH_SEQUENCES, SEQUENCE_LENGTH, ATTENTION_HEADS * head_width).astype(jnp.bfloat16)


def steps_of(stream_key, shape, cuts, low, largest):
    loudness, own = 1.0, jax.random.fold_in(stream_key, 6)
    for dim, blocks in cuts:
        steps = jnp.exp(jax.random.uniform(jax.random.fold_in(own, dim), (blocks,), jnp.float32, low / len(cuts), largest / len(cuts)))
        loudness = loudness * jnp.repeat(steps, shape[dim] // blocks).reshape([-1 if axis == dim else 1 for axis in range(len(shape))])
    return loudness


def routed_block(rng, own, number, rows, amount, top, bound, slope):
    sequence = jax.random.permutation(rng, amount)
    heavy_load, common = shares(amount, rows * top, bound, slope, True), shares(amount, rows * top, bound, slope, False)
    places = jnp.arange(amount)

    def named(tallies, offset_by):
        used = int((tallies > 0).sum())
        fixed = max(1, used // 4)
        moved = fixed + (places - fixed + offset_by * (used - fixed)) % max(1, amount - fixed)
        return jnp.zeros((amount,), jnp.int32).at[sequence[jnp.where(places < fixed, places, moved)]].set(jnp.asarray(tallies, jnp.int32))

    tallies = jnp.where(number % 4 == 0, named(heavy_load, number // 4), named(common, number - number // 4 - 1))
    mixed = jax.random.permutation(jax.random.fold_in(own, 3), amount)
    source_of, sink = mixed[0:amount // 2 * 2:2], mixed[1:amount // 2 * 2:2]
    slack = jnp.minimum(tallies[source_of] - 1, bound - tallies[sink]) // 2
    slack = jnp.where((source_of == sequence[0]) | (sink == sequence[0]) | (tallies[sink] == 0), 0, jnp.maximum(slack, 0))
    moved = jax.random.randint(jax.random.fold_in(own, 4), (amount // 2,), 0, 1 << 20) % (slack + 1)
    tallies = tallies.at[source_of].add(-moved).at[sink].add(moved)
    labels = jnp.searchsorted(jnp.cumsum(tallies), jnp.arange(rows * top), side="right").astype(jnp.int32)
    grid = labels.reshape(top, rows).T
    grid = grid[jax.random.permutation(jax.random.fold_in(own, 1), rows)]
    offset_by = jax.random.randint(jax.random.fold_in(own, 2), (rows, 1), 0, top)
    return jnp.take_along_axis(grid, (jnp.arange(top)[None, :] + offset_by) % top, axis=1)


def shares(number_of, total, limit, slope, full):
    portions = [(1 << 20) // math.isqrt(rank ** slope) + 1 for rank in range(1, number_of + 1)]
    largest = limit if full else min(limit, max(-(-total // number_of), total * portions[0] // sum(portions)))
    least = 1 if total - largest >= number_of - 1 else 0
    counts, surplus = [largest] + [least] * (number_of - 1), total - largest - least * (number_of - 1)
    while surplus > 0:
        candidates = [i for i in range(1, number_of) if counts[i] < largest] or [i for i in range(1, number_of) if counts[i] < limit]
        whole, budget = sum([portions[i] for i in candidates]), surplus
        for i in candidates:
            more = min(limit - counts[i], max(1, budget * portions[i] // whole), surplus)
            counts[i] = counts[i] + more
            surplus = surplus - more
    return np.array(counts)


def scatter_about(stream_key, dims, width, reach, shards=(), kind=jnp.bfloat16):
    values = width * jax.random.normal(stream_key, dims, jnp.float32)
    if shards:
        values = values * steps_of(stream_key, dims, shards, -0.22, 0.18)
    return jnp.clip(values, -reach, reach).astype(kind)


def setup_inputs(seed: int = 0) -> dict:
    splits = jax.random.split(jax.random.key(seed), 21)
    hidden_in = scatter_about(splits[0], (BATCH_SEQUENCES, SEQUENCE_LENGTH, D), 1.0, 6.0, ((0, 8), (1, 16)))
    queries = draw_queries(jax.random.fold_in(splits[20], 71), 0)
    key_value_latent = scatter_about(splits[2], (BATCH_SEQUENCES, SEQUENCE_LENGTH, LATENT_WIDTH), 1.0, 6.0, ((0, 8), (1, 16)))
    keys_rope = draw_keys_rope(jax.random.fold_in(splits[20], 71), 0)
    latent_norm_gain = jnp.clip(1.0 + 0.18 * jax.random.normal(splits[4], (LATENT_WIDTH,), jnp.float32), 0.1, 1.9)
    latent_up_weight = scatter_about(splits[5], (LATENT_WIDTH, ATTENTION_HEADS * (PLAIN_HEAD_WIDTH + VALUE_HEAD_WIDTH)), LATENT_WIDTH ** -0.5, 0.25)
    attn_gain = jnp.clip(1.0 + 0.18 * jax.random.normal(splits[6], (D_ATTN,), jnp.float32), 0.1, 1.9)
    out_proj = scatter_about(splits[7], (D_ATTN, D), D_ATTN ** -0.5, 0.1875)
    norm1_gain = jnp.clip(1.0 + 0.18 * jax.random.normal(splits[8], (D,), jnp.float32), 0.1, 1.9)
    norm1_bias = scatter_about(splits[9], (D,), 0.3, 1.5, (), jnp.float32)
    expert_ids_keys = jax.random.split(jax.random.fold_in(splits[10], 1), BATCH_SEQUENCES * SEQUENCE_LENGTH // TOK_DEV)
    expert_ids_turns = jax.random.permutation(jax.random.fold_in(splits[10], 3), BATCH_SEQUENCES * SEQUENCE_LENGTH // TOK_DEV)
    expert_ids = jax.vmap(lambda own, number: routed_block(jax.random.fold_in(splits[10], 2), own, number, TOK_DEV, EXPERTS, TOP_K, CAP, 2))(expert_ids_keys, expert_ids_turns).reshape((BATCH_SEQUENCES, SEQUENCE_LENGTH, TOP_K))
    route_weights = jnp.clip(0.1 + 0.9 * jax.random.uniform(splits[11], (BATCH_SEQUENCES, SEQUENCE_LENGTH, TOP_K), jnp.float32) ** steps_of(splits[11], (BATCH_SEQUENCES, SEQUENCE_LENGTH, TOP_K), ((0, 8), (1, 16)), -0.2, 0.2), 0.1, 1.0)
    gate_proj = scatter_about(splits[12], (EXPERTS, D, D_EXPERT), D ** -0.5, 0.125, ((0, 128),))
    up_proj = scatter_about(splits[13], (EXPERTS, D, D_EXPERT), D ** -0.5, 0.125, ((0, 128),))
    down_proj = scatter_about(splits[14], (EXPERTS, D_EXPERT, D), D_EXPERT ** -0.5, 0.25, ((0, 128),))
    shared_gate = scatter_about(splits[15], (D, D_SHARED), D ** -0.5, 0.125)
    shared_up = scatter_about(splits[16], (D, D_SHARED), D ** -0.5, 0.125)
    shared_down = scatter_about(splits[17], (D_SHARED, D), D_SHARED ** -0.5, 0.25)
    norm2_gain = jnp.clip(1.0 + 0.18 * jax.random.normal(splits[18], (D,), jnp.float32), 0.1, 1.9)
    norm2_bias = scatter_about(splits[19], (D,), 0.3, 1.5, (), jnp.float32)
    return {"hidden_in": hidden_in, "queries": queries, "key_value_latent": key_value_latent, "keys_rope": keys_rope, "latent_norm_gain": latent_norm_gain, "latent_up_weight": latent_up_weight, "attn_gain": attn_gain, "out_proj": out_proj, "norm1_gain": norm1_gain, "norm1_bias": norm1_bias, "expert_ids": expert_ids, "route_weights": route_weights, "gate_proj": gate_proj, "up_proj": up_proj, "down_proj": down_proj, "shared_gate": shared_gate, "shared_up": shared_up, "shared_down": shared_down, "norm2_gain": norm2_gain, "norm2_bias": norm2_bias}


ALPHA = 2.0 ** 0.25
ROUTED = 2.5
THETA = 10000.0

def rms_scaled(values, scaling):
    widened = values.astype(jnp.float32)
    return widened * lax.rsqrt(lax.optimization_barrier(jnp.mean(widened * widened, axis=-1, keepdims=True)) + 1e-06) * scaling

def layer_norm(values, scaling, bias_add):
    centre = values - lax.optimization_barrier(jnp.mean(values, axis=-1, keepdims=True))
    spread = lax.optimization_barrier(jnp.mean(centre * centre, axis=-1, keepdims=True))
    return centre * lax.rsqrt(spread + 1e-05) * scaling + bias_add

def rotation_tables(positions, rot_width):
    frequency = THETA ** (-jnp.arange(0, rot_width, 2, dtype=jnp.float32) / rot_width)
    angles = positions.astype(jnp.float32)[:, None] * frequency[None, :]
    return (jnp.cos(angles), jnp.sin(angles))

def turn(values, cosine_table, sine_table):
    half_width = values.shape[-1] // 2
    first_half = values[..., :half_width]
    second_half = values[..., half_width:]
    return jnp.concatenate([first_half * cosine_table - second_half * sine_table, second_half * cosine_table + first_half * sine_table], axis=-1)

def attend(query, key_full, values):
    length = query.shape[0]
    span_rows = 512 if length % 512 == 0 else length
    block_count = length // span_rows
    blocks = query.reshape(block_count, span_rows, query.shape[1])
    key_pos = jnp.arange(length, dtype=jnp.int32)
    factor = 1.0 / math.sqrt(query.shape[1])

    def one_block(inputs):
        block_index, query_rows = inputs
        scores = jnp.dot(query_rows, key_full.T, preferred_element_type=jnp.float32) * factor
        query_pos = block_index * span_rows + jnp.arange(span_rows, dtype=jnp.int32)
        scores = jnp.where(key_pos[None, :] <= query_pos[:, None], scores, -jnp.inf)
        row_max = lax.optimization_barrier(jnp.max(scores, axis=-1, keepdims=True))
        weights = jnp.exp(scores - row_max)
        weights = (weights / lax.optimization_barrier(jnp.sum(weights, axis=-1, keepdims=True))).astype(jnp.bfloat16)
        return jnp.dot(weights, values, preferred_element_type=jnp.float32).astype(jnp.bfloat16)
    attended = lax.map(one_block, (jnp.arange(block_count, dtype=jnp.int32), blocks))
    return attended.reshape(length, values.shape[1])

def swiglu_rows(rows, gate_mat, up_mat, down_mat):
    gated = jnp.dot(rows, gate_mat, preferred_element_type=jnp.float32)
    lifted = jnp.dot(rows, up_mat, preferred_element_type=jnp.float32)
    inner = (jax.nn.silu(gated) * lifted).astype(jnp.bfloat16)
    return jnp.dot(inner, down_mat, preferred_element_type=jnp.float32)

def mixer_sequence(hidden_seq, query_seq, latent_seq, rope_seq, latent_norm_gain, latent_up_weight, attn_gain, out_proj, norm1_gain, norm1_bias):
    length = hidden_seq.shape[0]
    normed = rms_scaled(latent_seq, latent_norm_gain).astype(jnp.bfloat16)
    keys_values = jnp.dot(normed, latent_up_weight, preferred_element_type=jnp.float32).astype(jnp.bfloat16)
    keys_values = keys_values.reshape(length, ATTENTION_HEADS, PLAIN_HEAD_WIDTH + VALUE_HEAD_WIDTH)
    cosine_table, sine_table = rotation_tables(jnp.arange(length, dtype=jnp.int32), QK_ROPE)
    keys_turned = turn(rope_seq.astype(jnp.float32), cosine_table, sine_table).astype(jnp.bfloat16)
    query_heads = query_seq.reshape(length, ATTENTION_HEADS, PLAIN_HEAD_WIDTH + QK_ROPE)
    query_turned = turn(query_heads[..., PLAIN_HEAD_WIDTH:].astype(jnp.float32), cosine_table[:, None, :], sine_table[:, None, :]).astype(jnp.bfloat16)
    query_full = jnp.concatenate([query_heads[..., :PLAIN_HEAD_WIDTH], query_turned], axis=-1)
    key_full = jnp.concatenate([keys_values[..., :PLAIN_HEAD_WIDTH], jnp.broadcast_to(keys_turned[:, None, :], (length, ATTENTION_HEADS, QK_ROPE))], axis=-1)
    values_heads = keys_values[..., PLAIN_HEAD_WIDTH:]
    by_head = lax.map(lambda inputs: attend(inputs[0], inputs[1], inputs[2]), (jnp.moveaxis(query_full, 1, 0), jnp.moveaxis(key_full, 1, 0), jnp.moveaxis(values_heads, 1, 0)))
    attended = jnp.moveaxis(by_head, 0, 1).reshape(length, ATTENTION_HEADS * VALUE_HEAD_WIDTH)
    attn_normed = rms_scaled(attended, attn_gain).astype(jnp.bfloat16)
    mixed = jnp.dot(attn_normed, out_proj, preferred_element_type=jnp.float32)
    return layer_norm(ALPHA * hidden_seq.astype(jnp.float32) + mixed, norm1_gain, norm1_bias).astype(jnp.bfloat16)

def reference(hidden_in, queries, key_value_latent, keys_rope, latent_norm_gain, latent_up_weight, attn_gain, out_proj, norm1_gain, norm1_bias, expert_ids, route_weights, gate_proj, up_proj, down_proj, shared_gate, shared_up, shared_down, norm2_gain, norm2_bias):
    batch_count = hidden_in.shape[0]
    length = hidden_in.shape[1]
    firsts = [mixer_sequence(hidden_in[member], queries[member], key_value_latent[member], keys_rope[member], latent_norm_gain, latent_up_weight, attn_gain, out_proj, norm1_gain, norm1_bias) for member in range(batch_count)]
    first = jnp.concatenate(firsts, axis=0)
    total = first.shape[0]
    blocks = total // TOK_DEV
    entries = expert_ids.reshape(blocks, TOK_DEV * TOP_K).astype(jnp.int32)
    onehot = (entries[:, :, None] == jnp.arange(EXPERTS, dtype=jnp.int32)[None, None, :]).astype(jnp.int32)
    earlier = jnp.cumsum(onehot, axis=1).astype(jnp.int32) - onehot
    slots = lax.optimization_barrier(jnp.sum(earlier * onehot, axis=-1)).astype(jnp.int32)
    block_ids = jnp.arange(blocks, dtype=jnp.int32)[:, None]
    places = (entries * (blocks * CAP) + block_ids * CAP + slots).reshape(-1).astype(jnp.int32)
    owners = (jnp.arange(total * TOP_K, dtype=jnp.int32) // TOP_K).astype(jnp.int32)
    table = jnp.full((EXPERTS * blocks * CAP,), total, jnp.int32).at[places].set(owners)
    padded = jnp.concatenate([first, jnp.zeros((1, D), jnp.bfloat16)], axis=0)

    def expert_block(inputs):
        gate_mat, up_mat, down_mat, picks = inputs
        return swiglu_rows(padded[picks], gate_mat, up_mat, down_mat).astype(jnp.bfloat16)
    expert_out = lax.map(expert_block, (gate_proj, up_proj, down_proj, table.reshape(EXPERTS, blocks * CAP)))
    gathered = expert_out.reshape(EXPERTS * blocks * CAP, D)[places].reshape(total, TOP_K, D)
    weights = route_weights.reshape(total, TOP_K).astype(jnp.float32)
    gates = weights / lax.optimization_barrier(jnp.sum(weights, axis=-1, keepdims=True)) * ROUTED
    routed = jnp.zeros((total, D), jnp.float32)
    for column in range(TOP_K):
        routed = routed + gates[:, column:column + 1] * gathered[:, column].astype(jnp.float32)
    feed = routed + swiglu_rows(first, shared_gate, shared_up, shared_down)
    result = layer_norm(ALPHA * first.astype(jnp.float32) + feed, norm2_gain, norm2_bias).astype(jnp.bfloat16)
    return result.reshape(batch_count, length, D)
```

```python
import math

import jax
import jax.numpy as jnp
from jax import lax
from jax.experimental import pallas as pl
from jax.experimental.pallas import tpu as pltpu
from jax.sharding import PartitionSpec as P

D = 2048
ATTENTION_HEADS = 16
PLAIN_HEAD_WIDTH = 64
QK_ROPE = 32
VALUE_HEAD_WIDTH = 64
TOP_K = 4


ALPHA = 2.0**0.25
ROUTED = 2.5
THETA = 10000.0


def copy_for_each(value, axis):
    size = lax.axis_size(axis)
    return lax.all_to_all(
        jnp.broadcast_to(value[None], (size, *value.shape)), axis, 0, 0, tiled=True
    )


def in_order(tiles, dim):
    lengths = list(tiles.shape[1:])
    lengths[dim] *= tiles.shape[0]
    return jnp.moveaxis(tiles, 0, dim).reshape(lengths)


def collect(value, axis, dim):
    tiles = copy_for_each(value, axis)
    return in_order(tiles, dim)


def rms_scaled(values, scaling):
    widened = values.astype(jnp.float32)
    return (
        widened * lax.rsqrt(jnp.mean(widened * widened, axis=-1, keepdims=True) + 1e-06) * scaling
    )


def layer_norm(values, scaling, bias_add):
    centre = values - jnp.mean(values, axis=-1, keepdims=True)
    spread = jnp.mean(centre * centre, axis=-1, keepdims=True)
    return centre * lax.rsqrt(spread + 1e-05) * scaling + bias_add


def rotation_tables(positions, rot_width):
    frequency = THETA ** (-jnp.arange(0, rot_width, 2, dtype=jnp.float32) / rot_width)
    angles = positions.astype(jnp.float32)[:, None] * frequency[None, :]
    return (jnp.cos(angles), jnp.sin(angles))


def turn(values, cosine_table, sine_table):
    half_width = values.shape[-1] // 2
    first_half = values[..., :half_width]
    second_half = values[..., half_width:]
    return jnp.concatenate(
        [
            first_half * cosine_table - second_half * sine_table,
            second_half * cosine_table + first_half * sine_table,
        ],
        axis=-1,
    )


def attend(query, key_full, values):
    length = query.shape[0]
    span_rows = 512
    block_count = length // span_rows
    blocks = query.reshape(block_count, span_rows, query.shape[1])
    key_pos = jnp.arange(length, dtype=jnp.int32)
    factor = 1.0 / math.sqrt(query.shape[1])

    def one_block(inputs):
        block_index, query_rows = inputs
        scores = jnp.dot(query_rows, key_full.T, preferred_element_type=jnp.float32) * factor
        query_pos = block_index * span_rows + jnp.arange(span_rows, dtype=jnp.int32)
        scores = jnp.where(key_pos[None, :] <= query_pos[:, None], scores, -jnp.inf)
        row_max = jnp.max(scores, axis=-1, keepdims=True)
        weights = jnp.exp(scores - row_max)
        weights = (weights / jnp.sum(weights, axis=-1, keepdims=True)).astype(jnp.bfloat16)
        return jnp.dot(weights, values, preferred_element_type=jnp.float32).astype(jnp.bfloat16)

    attended = lax.map(one_block, (jnp.arange(block_count, dtype=jnp.int32), blocks))
    return attended.reshape(length, values.shape[1])


MESH = pl.DeviceIdType.MESH
GROUPS = 8
PER_GROUP = 16
SLOTS = 6
GROUP_ROWS = PER_GROUP * SLOTS
TILES = D // 128


def position_of(sp, dp):
    return sp // 4, sp % 4, dp // 2, dp % 2


def step_of(k):
    dc, dy, dx = (k // 16) % 2, (k // 4) % 4, k % 4
    return (k // 32 + 8 - dx - dy) % 4, dy, dx, dc


def device_at(here, k, sign):
    z, y, x, c = here
    dz, dy, dx, dc = step_of(k)
    z, y = (z + 4 + sign * dz) % 4, (y + 4 + sign * dy) % 4
    x, c = (x + 4 + sign * dx) % 4, (c + dc) % 2
    return (z * 4 + y, x * 2 + c)


def order_of(expert_ids, here):
    z, y, x, c = here
    ez, ey, ex, ec = expert_ids // 32, (expert_ids // 8) % 4, (expert_ids // 2) % 4, expert_ids % 2
    dz, dy, dx, dc = (ez - z) & 3, (ey - y) & 3, (ex - x) & 3, (ec + c) & 1
    return (((dz + dy + dx) & 3) * 2 + dc) * 16 + dy * 4 + dx


def iota(shape, dim):
    return lax.broadcasted_iota(jnp.int32, shape, dim)


def experts_kernel(
    ids_ref, ids_t_ref, weights_ref, attended_ref, attn_gain_ref, hidden_ref,
    gain1_ref, bias1_ref, gain2_ref, bias2_ref,
    out_proj_hbm, gate_hbm, up_hbm, down_hbm, sgate_hbm, sup_hbm, sdown_hbm,
    out_ref,
    out_proj, gate, up, down, sgate, sup, sdown,
    first, places_t, places, gates, send, arrived, made, returned, flat, rows, total,
    load_sem, send_sem, recv_sem, back_sem, ret_sem,
):
    here = position_of(lax.axis_index("sp"), lax.axis_index("dp"))
    loads = [
        pltpu.make_async_copy(src, dst, load_sem.at[i])
        for i, (src, dst) in enumerate(
            (
                (out_proj_hbm, out_proj), (sgate_hbm, sgate), (sup_hbm, sup), (sdown_hbm, sdown),
                (gate_hbm.at[0], gate), (up_hbm.at[0], up), (down_hbm.at[0], down),
            )
        )
    ]
    for load in loads:
        load.start()
    barrier = pltpu.get_barrier_semaphore()

    def greet(k, carry):
        pl.semaphore_signal(barrier, inc=1, device_id=device_at(here, k, 1), device_id_type=MESH)
        return carry

    lax.fori_loop(1, 128, greet, 0)

    ids_t = ids_t_ref[...]
    named_t = jnp.zeros((128, 128), jnp.bool_)
    for col in range(TOP_K):
        named_t = named_t | (iota((128, 128), 0) == ids_t[col : col + 1, :])
    before = (iota((128, 128), 0) < iota((128, 128), 1)).astype(jnp.bfloat16)
    count_t = jnp.dot(named_t.astype(jnp.bfloat16), before, preferred_element_type=jnp.float32)
    order_t = order_of(ids_t, here)
    for col in range(TOP_K):
        slot = jnp.sum(
            jnp.where(iota((128, 128), 0) == ids_t[col : col + 1, :], count_t, 0.0),
            axis=0, keepdims=True,
        )
        places_t[col : col + 1, :] = order_t[col : col + 1, :] * SLOTS + slot.astype(jnp.int32)
    ids = ids_ref[...]
    named = jnp.zeros((128, 128), jnp.bool_)
    for col in range(TOP_K):
        named = named | (iota((128, 128), 1) == ids[:, col : col + 1])
    after = (iota((128, 128), 1) < iota((128, 128), 0)).astype(jnp.bfloat16)
    count = jnp.dot(after, named.astype(jnp.bfloat16), preferred_element_type=jnp.float32)
    order = order_of(ids, here)
    for col in range(TOP_K):
        slot = jnp.sum(
            jnp.where(iota((128, 128), 1) == ids[:, col : col + 1], count, 0.0),
            axis=1, keepdims=True,
        )
        places[:, col : col + 1] = order[:, col : col + 1] * SLOTS + slot.astype(jnp.int32)
    weights = weights_ref[...]
    gates[...] = weights / jnp.sum(weights, axis=-1, keepdims=True) * ROUTED

    attn_normed = rms_scaled(attended_ref[...], attn_gain_ref[...]).astype(jnp.bfloat16)
    loads[0].wait()
    mixed = jnp.dot(attn_normed, out_proj[...], preferred_element_type=jnp.float32)
    first[...] = layer_norm(
        ALPHA * hidden_ref[...].astype(jnp.float32) + mixed, gain1_ref[...], bias1_ref[...]
    ).astype(jnp.bfloat16)

    def pack(group, source, target):
        for tile in range(TILES):
            flat[pl.ds(tile, GROUP_ROWS, stride=TILES), :] = source[:, tile * 128 : tile * 128 + 128]
        target[pl.ds(group * PER_GROUP, PER_GROUP)] = (
            flat[...].astype(jnp.bfloat16).reshape(PER_GROUP, SLOTS * TILES, 128)
        )

    def unpack(group, source):
        flat[...] = (
            source[pl.ds(group * PER_GROUP, PER_GROUP)]
            .reshape(GROUP_ROWS * TILES, 128)
            .astype(jnp.float32)
        )
        for tile in range(TILES):
            rows[:, tile * 128 : tile * 128 + 128] = flat[
                pl.ds(tile, GROUP_ROWS, stride=TILES), :
            ].astype(jnp.bfloat16)

    def dispatch(k, carry):
        pltpu.make_async_remote_copy(
            send.at[k], arrived.at[k], send_sem, recv_sem.at[k // PER_GROUP],
            device_id=device_at(here, k, 1), device_id_type=MESH,
        ).start()
        return carry

    def reply(k, carry):
        pltpu.make_async_remote_copy(
            made.at[k], returned.at[k], back_sem, ret_sem.at[k // PER_GROUP],
            device_id=device_at(here, k, -1), device_id_type=MESH,
        ).start()
        return carry

    def wait_blocks(group, buffer, sem):
        @pl.when(group == 0)
        def _():
            block = buffer.at[pl.ds(0, PER_GROUP - 1)]
            pltpu.make_async_copy(block, block, sem.at[group]).wait()

        @pl.when(group > 0)
        def _():
            block = buffer.at[pl.ds(0, PER_GROUP)]
            pltpu.make_async_copy(block, block, sem.at[group]).wait()

    def load_group(group, carry):
        picks = iota((GROUP_ROWS, 128), 0) + group * GROUP_ROWS
        chosen = jnp.zeros((GROUP_ROWS, 128), jnp.bool_)
        for col in range(TOP_K):
            chosen = chosen | (picks == places_t[col : col + 1, :])
        out = jnp.dot(
            chosen.astype(jnp.bfloat16), first[...], preferred_element_type=jnp.float32
        )
        pack(group, out, send)

        @pl.when(group == 0)
        def _():
            pl.semaphore_wait(barrier, 127)

        lax.fori_loop(jnp.maximum(group * PER_GROUP, 1), (group + 1) * PER_GROUP, dispatch, 0)
        return carry

    lax.fori_loop(0, GROUPS, load_group, 0)
    arrived[0] = send[0]

    for load in loads[1:4]:
        load.wait()
    tokens = first[...]
    gated = jnp.dot(tokens, sgate[...], preferred_element_type=jnp.float32)
    lifted = jnp.dot(tokens, sup[...], preferred_element_type=jnp.float32)
    inner = (gated / (1.0 + jnp.exp(-gated)) * lifted).astype(jnp.bfloat16)
    total[...] = ALPHA * tokens.astype(jnp.float32) + jnp.dot(
        inner, sdown[...], preferred_element_type=jnp.float32
    )
    for load in loads[4:]:
        load.wait()

    def expert_group(group, carry):
        wait_blocks(group, arrived, recv_sem)
        unpack(group, arrived)
        tokens = rows[...]
        gated = jnp.dot(tokens, gate[...], preferred_element_type=jnp.float32)
        lifted = jnp.dot(tokens, up[...], preferred_element_type=jnp.float32)
        inner = (gated / (1.0 + jnp.exp(-gated)) * lifted).astype(jnp.bfloat16)
        out = jnp.dot(inner, down[...], preferred_element_type=jnp.float32)
        pack(group, out, made)
        lax.fori_loop(jnp.maximum(group * PER_GROUP, 1), (group + 1) * PER_GROUP, reply, 0)
        return carry

    lax.fori_loop(0, GROUPS, expert_group, 0)
    returned[0] = made[0]

    def combine_group(group, carry):
        wait_blocks(group, returned, ret_sem)
        unpack(group, returned)
        picks = iota((128, GROUP_ROWS), 1) + group * GROUP_ROWS
        share = jnp.zeros((128, GROUP_ROWS), jnp.float32)
        for col in range(TOP_K):
            share = share + jnp.where(
                picks == places[:, col : col + 1], gates[:, col : col + 1], 0.0
            )
        high = share.astype(jnp.bfloat16)
        low = (share - high.astype(jnp.float32)).astype(jnp.bfloat16)
        tokens = rows[...]
        total[...] += jnp.dot(high, tokens, preferred_element_type=jnp.float32) + jnp.dot(
            low, tokens, preferred_element_type=jnp.float32
        )
        return carry

    lax.fori_loop(0, GROUPS, combine_group, 0)
    out_ref[...] = layer_norm(total[...], gain2_ref[...], bias2_ref[...]).astype(jnp.bfloat16)
    sent = send.at[pl.ds(0, 127)]
    pltpu.make_async_copy(sent, sent, send_sem).wait()
    pltpu.make_async_copy(sent, sent, back_sem).wait()


def experts_layer(
    ids, ids_t, weights, attended, attn_gain, hidden, gain1, bias1, gain2, bias2,
    out_proj, gate_proj, up_proj, down_proj, shared_gate, shared_up, shared_down,
):
    bf16, f32 = jnp.bfloat16, jnp.float32
    vmem = pl.BlockSpec(memory_space=pltpu.VMEM)
    hbm = pl.BlockSpec(memory_space=pl.ANY)
    blocks = pltpu.VMEM((GROUPS * PER_GROUP, SLOTS * TILES, 128), bf16)
    return pl.pallas_call(
        experts_kernel,
        out_shape=jax.ShapeDtypeStruct((128, D), bf16),
        in_specs=[vmem] * 10 + [hbm] * 7,
        out_specs=vmem,
        scratch_shapes=[
            pltpu.VMEM((1024, D), bf16),
            pltpu.VMEM((D, 512), bf16),
            pltpu.VMEM((D, 512), bf16),
            pltpu.VMEM((512, D), bf16),
            pltpu.VMEM((D, 512), bf16),
            pltpu.VMEM((D, 512), bf16),
            pltpu.VMEM((512, D), bf16),
            pltpu.VMEM((128, D), bf16),
            pltpu.VMEM((TOP_K, 128), jnp.int32),
            pltpu.VMEM((128, TOP_K), jnp.int32),
            pltpu.VMEM((128, TOP_K), f32),
            blocks, blocks, blocks, blocks,
            pltpu.VMEM((GROUP_ROWS * TILES, 128), f32),
            pltpu.VMEM((GROUP_ROWS, D), bf16),
            pltpu.VMEM((128, D), f32),
            pltpu.SemaphoreType.DMA((7,)),
            pltpu.SemaphoreType.DMA,
            pltpu.SemaphoreType.DMA((GROUPS,)),
            pltpu.SemaphoreType.DMA,
            pltpu.SemaphoreType.DMA((GROUPS,)),
        ],
        compiler_params=pltpu.CompilerParams(
            collective_id=1, has_side_effects=True, vmem_limit_bytes=56 * 2**20
        ),
    )(
        ids, ids_t, weights, attended, attn_gain, hidden, gain1, bias1, gain2, bias2,
        out_proj, gate_proj, up_proj, down_proj, shared_gate, shared_up, shared_down,
    )


def per_device(
    hidden_in,
    queries,
    key_value_latent,
    keys_rope,
    latent_norm_gain,
    latent_up_weight,
    attn_gain,
    out_proj,
    norm1_gain,
    norm1_bias,
    expert_ids,
    route_weights,
    gate_proj,
    up_proj,
    down_proj,
    shared_gate,
    shared_up,
    shared_down,
    norm2_gain,
    norm2_bias,
):
    seq_devices = lax.axis_size("sp")
    tok_rows = hidden_in.shape[1]
    length = tok_rows * seq_devices
    heads_here = ATTENTION_HEADS // seq_devices
    normed = rms_scaled(key_value_latent[0], latent_norm_gain).astype(jnp.bfloat16)
    keys_values = jnp.dot(normed, latent_up_weight, preferred_element_type=jnp.float32).astype(
        jnp.bfloat16
    )
    local_pos = lax.axis_index("sp") * tok_rows + jnp.arange(tok_rows, dtype=jnp.int32)
    cos_local, sin_local = rotation_tables(local_pos, QK_ROPE)
    keys_turned = turn(keys_rope[0].astype(jnp.float32), cos_local, sin_local).astype(jnp.bfloat16)
    query_send = queries[0].reshape(
        tok_rows, seq_devices, heads_here * (PLAIN_HEAD_WIDTH + QK_ROPE)
    )
    pair_send = keys_values.reshape(
        tok_rows, seq_devices, heads_here * (PLAIN_HEAD_WIDTH + VALUE_HEAD_WIDTH)
    )
    query_heads, pair_heads = (
        lax.all_to_all(query_send, "sp", split_axis=1, concat_axis=0, tiled=True),
        lax.all_to_all(pair_send, "sp", split_axis=1, concat_axis=0, tiled=True),
    )
    keys_whole = collect(keys_turned, "sp", 0)
    cos_whole, sin_whole = rotation_tables(jnp.arange(length, dtype=jnp.int32), QK_ROPE)
    query_turned = turn(
        query_heads[..., PLAIN_HEAD_WIDTH:].astype(jnp.float32),
        cos_whole[:, None, :],
        sin_whole[:, None, :],
    ).astype(jnp.bfloat16)
    query_full = jnp.concatenate([query_heads[..., :PLAIN_HEAD_WIDTH], query_turned], axis=-1)
    key_full = jnp.concatenate(
        [pair_heads[..., :PLAIN_HEAD_WIDTH], keys_whole[:, None, :]], axis=-1
    )
    values_heads = pair_heads[..., PLAIN_HEAD_WIDTH:]
    by_head = lax.map(
        lambda inputs: attend(inputs[0], inputs[1], inputs[2]),
        (
            jnp.moveaxis(query_full, 1, 0),
            jnp.moveaxis(key_full, 1, 0),
            jnp.moveaxis(values_heads, 1, 0),
        ),
    )
    outgoing = jnp.moveaxis(by_head, 0, 1).reshape(
        seq_devices, tok_rows, heads_here * VALUE_HEAD_WIDTH
    )
    incoming = lax.all_to_all(outgoing, "sp", split_axis=0, concat_axis=2, tiled=True)
    ids = expert_ids[0]
    result = experts_layer(
        ids, ids.T, route_weights[0], incoming[0], attn_gain[None], hidden_in[0],
        norm1_gain[None], norm1_bias[None], norm2_gain[None], norm2_bias[None],
        out_proj, gate_proj, up_proj, down_proj, shared_gate, shared_up, shared_down,
    )
    return result.reshape(1, tok_rows, D)


def solution(mesh):
    in_specs = (
        P("dp", "sp", None),
        P("dp", "sp", None),
        P("dp", "sp", None),
        P("dp", "sp", None),
        P(),
        P(),
        P(),
        P(),
        P(),
        P(),
        P("dp", "sp", None),
        P("dp", "sp", None),
        P(("sp", "dp"), None, None),
        P(("sp", "dp"), None, None),
        P(("sp", "dp"), None, None),
        P(),
        P(),
        P(),
        P(),
        P(),
    )
    out_specs = P("dp", "sp", None)
    return jax.shard_map(
        per_device, mesh=mesh, in_specs=in_specs, out_specs=out_specs, check_vma=False
    )
```

```python
import math

import jax
import jax.numpy as jnp
import numpy as np
from jax import lax
from jax.experimental import pallas as pl
from jax.experimental.pallas import tpu as pltpu
from jax.sharding import PartitionSpec as P

D = 2048
ATTENTION_HEADS = 16
PLAIN_HEAD_WIDTH = 64
QK_ROPE = 32
VALUE_HEAD_WIDTH = 64
TOP_K = 4


ALPHA = 2.0**0.25
ROUTED = 2.5
THETA = 10000.0


def rms_scaled(values, scaling):
    widened = values.astype(jnp.float32)
    return (
        widened * lax.rsqrt(jnp.mean(widened * widened, axis=-1, keepdims=True) + 1e-06) * scaling
    )


def layer_norm(values, scaling, bias_add):
    centre = values - jnp.mean(values, axis=-1, keepdims=True)
    spread = jnp.mean(centre * centre, axis=-1, keepdims=True)
    return centre * lax.rsqrt(spread + 1e-05) * scaling + bias_add


def rotation_tables(devices, rows):
    frequency = np.power(THETA, -np.arange(0, QK_ROPE, 2) / QK_ROPE).astype(np.float32)
    positions = np.arange(devices * rows, dtype=np.float32).reshape(devices, 1, rows)
    angles = (positions * frequency[None, :, None]).astype(np.float64)
    return np.concatenate([np.cos(angles), np.sin(angles)], axis=1).astype(np.float32)


MESH = pl.DeviceIdType.MESH
GROUPS = 8
PER_GROUP = 16
SLOTS = 6
GROUP_ROWS = PER_GROUP * SLOTS
TILES = D // 128


def position_of(sp, dp):
    return sp // 4, sp % 4, dp // 2, dp % 2


def step_of(k):
    dc, dy, dx = (k // 16) % 2, (k // 4) % 4, k % 4
    return (k // 32 + 8 - dx - dy) % 4, dy, dx, dc


def peer_at(here, k):
    z, y = here[:2]
    dy = k % 4
    return (z + (k // 4 + 4 - dy)) % 4 * 4 + (y + dy) % 4


def device_at(here, k, sign):
    z, y, x, c = here
    dz, dy, dx, dc = step_of(k)
    z, y = (z + 4 + sign * dz) % 4, (y + 4 + sign * dy) % 4
    x, c = (x + 4 + sign * dx) % 4, (c + dc) % 2
    return (z * 4 + y, x * 2 + c)


def order_of(expert_ids, here):
    z, y, x, c = here
    ez, ey, ex, ec = expert_ids // 32, (expert_ids // 8) % 4, (expert_ids // 2) % 4, expert_ids % 2
    dz, dy, dx, dc = (ez - z) & 3, (ey - y) & 3, (ex - x) & 3, (ec + c) & 1
    return (((dz + dy + dx) & 3) * 2 + dc) * 16 + dy * 4 + dx


def iota(shape, dim):
    return lax.broadcasted_iota(jnp.int32, shape, dim)


def layer_kernel(
    ids_ref, ids_t_ref, weights_ref, rope_ref, latent_gain_ref, attn_gain_ref,
    gain1_ref, bias1_ref, gain2_ref, bias2_ref,
    latent_hbm, latent_up_hbm, queries_hbm, tables_hbm, hidden_hbm,
    out_proj_hbm, gate_hbm, up_hbm, down_hbm, sgate_hbm, sup_hbm, sdown_hbm,
    out_ref,
    latent, latent_up, queries, tables, hidden,
    out_proj, gate, up, down, sgate, sup, sdown,
    turned, message, letters, keys, asked, values_t, scores, heads_out, heads_in,
    first, places_t, places, gates, send, arrived, made, returned, flat, rows, total,
    load_sem, msg_sem, letter_sem, head_sem, heads_sem,
    send_sem, recv_sem, back_sem, ret_sem,
):
    sp, dp = lax.axis_index("sp"), lax.axis_index("dp")
    here = position_of(sp, dp)
    loads = [
        pltpu.make_async_copy(src, dst, load_sem.at[i])
        for i, (src, dst) in enumerate(
            (
                (latent_hbm, latent), (latent_up_hbm, latent_up), (queries_hbm, queries),
                (tables_hbm.at[sp], tables), (hidden_hbm, hidden), (out_proj_hbm, out_proj),
                (sgate_hbm, sgate), (sup_hbm, sup), (sdown_hbm, sdown),
                (gate_hbm.at[0], gate), (up_hbm.at[0], up), (down_hbm.at[0], down),
            )
        )
    ]
    for load in loads:
        load.start()
    barrier = pltpu.get_barrier_semaphore()

    def greet(k, carry):
        pl.semaphore_signal(barrier, inc=1, device_id=device_at(here, k, 1), device_id_type=MESH)
        return carry

    lax.fori_loop(1, 128, greet, 0)

    loads[3].wait()
    cosine, sine = tables[0:16, :], tables[16:32, :]

    def turn(both):
        a, b = both[0:16].astype(jnp.float32), both[16:32].astype(jnp.float32)
        return jnp.concatenate([a * cosine - b * sine, b * cosine + a * sine], axis=0).astype(
            jnp.bfloat16
        )

    rope = jnp.concatenate(
        [rope_ref[...].astype(jnp.float32), jnp.zeros((128, 96), jnp.float32)], axis=1
    )
    rope_t = turn(rope.T[0:32])
    loads[2].wait()
    for tile in range(12):
        turned[tile * 128 : tile * 128 + 128, :] = queries[:, tile * 128 : tile * 128 + 128].T
    for head in range(16):
        block = turned[head * 96 : head * 96 + 96, :]
        message[head, 0:64, :] = block[0:64]
        message[head, 64:96, :] = turn(block[64:96])
        message[head, 96:128, :] = rope_t
    loads[0].wait()
    normed = rms_scaled(latent[...], latent_gain_ref[...]).astype(jnp.bfloat16)
    loads[1].wait()
    keys_values = jnp.dot(normed, latent_up[...], preferred_element_type=jnp.float32).astype(
        jnp.bfloat16
    )
    for head in range(16):
        message[head, 128:256, :] = keys_values[:, head * 128 : head * 128 + 128]
    pl.semaphore_wait(barrier, 127)

    def deliver(k, carry):
        peer = peer_at(here, k)
        pltpu.make_async_remote_copy(
            message.at[peer], letters.at[sp], msg_sem, letter_sem,
            device_id=(peer, dp), device_id_type=MESH,
        ).start()
        return carry

    lax.fori_loop(1, 16, deliver, 0)
    letters[sp] = message[sp]

    ids_t = ids_t_ref[...]
    named_t = jnp.zeros((128, 128), jnp.bool_)
    for col in range(TOP_K):
        named_t = named_t | (iota((128, 128), 0) == ids_t[col : col + 1, :])
    before = (iota((128, 128), 0) < iota((128, 128), 1)).astype(jnp.bfloat16)
    count_t = jnp.dot(named_t.astype(jnp.bfloat16), before, preferred_element_type=jnp.float32)
    order_t = order_of(ids_t, here)
    for col in range(TOP_K):
        slot = jnp.sum(
            jnp.where(iota((128, 128), 0) == ids_t[col : col + 1, :], count_t, 0.0),
            axis=0, keepdims=True,
        )
        places_t[col : col + 1, :] = order_t[col : col + 1, :] * SLOTS + slot.astype(jnp.int32)
    ids = ids_ref[...]
    named = jnp.zeros((128, 128), jnp.bool_)
    for col in range(TOP_K):
        named = named | (iota((128, 128), 1) == ids[:, col : col + 1])
    after = (iota((128, 128), 1) < iota((128, 128), 0)).astype(jnp.bfloat16)
    count = jnp.dot(after, named.astype(jnp.bfloat16), preferred_element_type=jnp.float32)
    order = order_of(ids, here)
    for col in range(TOP_K):
        slot = jnp.sum(
            jnp.where(iota((128, 128), 1) == ids[:, col : col + 1], count, 0.0),
            axis=1, keepdims=True,
        )
        places[:, col : col + 1] = order[:, col : col + 1] * SLOTS + slot.astype(jnp.int32)
    weights = weights_ref[...]
    gates[...] = weights / jnp.sum(weights, axis=-1, keepdims=True) * ROUTED

    asked[...] = jnp.zeros_like(asked)
    fifteen = message.at[pl.ds(0, 15)]
    pltpu.make_async_copy(fifteen, fifteen, letter_sem).wait()
    for block in range(16):
        span = slice(block * 128, block * 128 + 128)
        top, pair = letters[block, 0:128, :], letters[block, 128:256, :]
        keys[span, 0:128] = pair
        keys[span, 128:256] = top.T
        asked[0:64, span] = top[0:64]
        asked[224:256, span] = top[64:96]
        values_t[:, span] = pair.T

    factor = math.log2(math.e) / math.sqrt(PLAIN_HEAD_WIDTH + QK_ROPE)

    def attend(index):
        asking = asked[:, index * 256 : index * 256 + 256]
        peak = None
        for other in range(index + 1):
            span = slice(other * 256, other * 256 + 256)
            part = jnp.dot(keys[span, :], asking, preferred_element_type=jnp.float32)
            if other == index:
                part = jnp.where(iota((256, 256), 0) <= iota((256, 256), 1), part, -jnp.inf)
            scores[span, :] = part
            high = jnp.max(part, axis=0, keepdims=True)
            peak = high if peak is None else jnp.maximum(peak, high)
        peak = peak * factor
        weight, mixed = 0.0, 0.0
        for other in range(index + 1):
            span = slice(other * 256, other * 256 + 256)
            part = jnp.exp2(scores[span, :] * factor - peak)
            weight = weight + jnp.sum(part, axis=0, keepdims=True)
            mixed = mixed + jnp.dot(
                values_t[64:128, span], part.astype(jnp.bfloat16),
                preferred_element_type=jnp.float32,
            )
        mixed = (mixed / weight).astype(jnp.bfloat16)
        heads_out[2 * index] = mixed[:, 0:128]
        heads_out[2 * index + 1] = mixed[:, 128:256]

    def give_back(base):
        def give(k, carry):
            peer = base + (sp + k) % 8

            @pl.when(peer != sp)
            def _():
                pltpu.make_async_remote_copy(
                    heads_out.at[peer], heads_in.at[sp], head_sem, heads_sem,
                    device_id=(peer, dp), device_id_type=MESH,
                ).start()

            return carry

        lax.fori_loop(0, 8, give, 0)

    for index in (7, 6, 5, 4):
        attend(index)
    give_back(8)
    for index in (3, 2, 1, 0):
        attend(index)
    give_back(0)
    heads_in[sp] = heads_out[sp]
    loads[4].wait()
    loads[5].wait()
    arrivals = heads_out.at[pl.ds(0, 15)]
    pltpu.make_async_copy(arrivals, arrivals, heads_sem).wait()
    attended = heads_in[...].reshape(1024, 128).T
    attn_normed = rms_scaled(attended, attn_gain_ref[...]).astype(jnp.bfloat16)
    mixed = jnp.dot(attn_normed, out_proj[...], preferred_element_type=jnp.float32)
    first[...] = layer_norm(
        ALPHA * hidden[...].astype(jnp.float32) + mixed, gain1_ref[...], bias1_ref[...]
    ).astype(jnp.bfloat16)

    def pack(group, source, target):
        for tile in range(TILES):
            flat[pl.ds(tile, GROUP_ROWS, stride=TILES), :] = source[:, tile * 128 : tile * 128 + 128]
        target[pl.ds(group * PER_GROUP, PER_GROUP)] = (
            flat[...].astype(jnp.bfloat16).reshape(PER_GROUP, SLOTS * TILES, 128)
        )

    def unpack(group, source):
        flat[...] = (
            source[pl.ds(group * PER_GROUP, PER_GROUP)]
            .reshape(GROUP_ROWS * TILES, 128)
            .astype(jnp.float32)
        )
        for tile in range(TILES):
            rows[:, tile * 128 : tile * 128 + 128] = flat[
                pl.ds(tile, GROUP_ROWS, stride=TILES), :
            ].astype(jnp.bfloat16)

    def dispatch(k, carry):
        pltpu.make_async_remote_copy(
            send.at[k], arrived.at[k], send_sem, recv_sem.at[k // PER_GROUP],
            device_id=device_at(here, k, 1), device_id_type=MESH,
        ).start()
        return carry

    def reply(k, carry):
        pltpu.make_async_remote_copy(
            made.at[k], returned.at[k], back_sem, ret_sem.at[k // PER_GROUP],
            device_id=device_at(here, k, -1), device_id_type=MESH,
        ).start()
        return carry

    def wait_blocks(group, buffer, sem):
        @pl.when(group == 0)
        def _():
            block = buffer.at[pl.ds(0, PER_GROUP - 1)]
            pltpu.make_async_copy(block, block, sem.at[group]).wait()

        @pl.when(group > 0)
        def _():
            block = buffer.at[pl.ds(0, PER_GROUP)]
            pltpu.make_async_copy(block, block, sem.at[group]).wait()

    def load_group(group, carry):
        picks = iota((GROUP_ROWS, 128), 0) + group * GROUP_ROWS
        chosen = jnp.zeros((GROUP_ROWS, 128), jnp.bool_)
        for col in range(TOP_K):
            chosen = chosen | (picks == places_t[col : col + 1, :])
        out = jnp.dot(
            chosen.astype(jnp.bfloat16), first[...], preferred_element_type=jnp.float32
        )
        pack(group, out, send)

        lax.fori_loop(jnp.maximum(group * PER_GROUP, 1), (group + 1) * PER_GROUP, dispatch, 0)
        return carry

    lax.fori_loop(0, GROUPS, load_group, 0)
    arrived[0] = send[0]

    for load in loads[6:9]:
        load.wait()
    tokens = first[...]
    gated = jnp.dot(tokens, sgate[...], preferred_element_type=jnp.float32)
    lifted = jnp.dot(tokens, sup[...], preferred_element_type=jnp.float32)
    inner = (gated / (1.0 + jnp.exp(-gated)) * lifted).astype(jnp.bfloat16)
    total[...] = ALPHA * tokens.astype(jnp.float32) + jnp.dot(
        inner, sdown[...], preferred_element_type=jnp.float32
    )
    for load in loads[9:]:
        load.wait()

    def expert_group(group, carry):
        wait_blocks(group, arrived, recv_sem)
        unpack(group, arrived)
        tokens = rows[...]
        gated = jnp.dot(tokens, gate[...], preferred_element_type=jnp.float32)
        lifted = jnp.dot(tokens, up[...], preferred_element_type=jnp.float32)
        inner = (gated / (1.0 + jnp.exp(-gated)) * lifted).astype(jnp.bfloat16)
        out = jnp.dot(inner, down[...], preferred_element_type=jnp.float32)
        pack(group, out, made)
        lax.fori_loop(jnp.maximum(group * PER_GROUP, 1), (group + 1) * PER_GROUP, reply, 0)
        return carry

    lax.fori_loop(0, GROUPS, expert_group, 0)
    returned[0] = made[0]

    def combine_group(group, carry):
        wait_blocks(group, returned, ret_sem)
        unpack(group, returned)
        picks = iota((128, GROUP_ROWS), 1) + group * GROUP_ROWS
        share = jnp.zeros((128, GROUP_ROWS), jnp.float32)
        for col in range(TOP_K):
            share = share + jnp.where(
                picks == places[:, col : col + 1], gates[:, col : col + 1], 0.0
            )
        high = share.astype(jnp.bfloat16)
        low = (share - high.astype(jnp.float32)).astype(jnp.bfloat16)
        tokens = rows[...]
        total[...] += jnp.dot(high, tokens, preferred_element_type=jnp.float32) + jnp.dot(
            low, tokens, preferred_element_type=jnp.float32
        )
        return carry

    lax.fori_loop(0, GROUPS, combine_group, 0)
    out_ref[...] = layer_norm(total[...], gain2_ref[...], bias2_ref[...]).astype(jnp.bfloat16)
    sent = send.at[pl.ds(0, 127)]
    pltpu.make_async_copy(sent, sent, send_sem).wait()
    pltpu.make_async_copy(sent, sent, back_sem).wait()
    pltpu.make_async_copy(fifteen, fifteen, msg_sem).wait()
    pltpu.make_async_copy(arrivals, arrivals, head_sem).wait()


def per_device(
    hidden_in, queries, key_value_latent, keys_rope, latent_norm_gain, latent_up_weight,
    attn_gain, out_proj, norm1_gain, norm1_bias, expert_ids, route_weights,
    gate_proj, up_proj, down_proj, shared_gate, shared_up, shared_down, norm2_gain, norm2_bias,
):
    bf16, f32 = jnp.bfloat16, jnp.float32
    vmem = pl.BlockSpec(memory_space=pltpu.VMEM)
    hbm = pl.BlockSpec(memory_space=pl.ANY)
    blocks = pltpu.VMEM((GROUPS * PER_GROUP, SLOTS * TILES, 128), bf16)
    tables = jnp.asarray(rotation_tables(16, 128))
    ids = expert_ids[0]
    result = pl.pallas_call(
        layer_kernel,
        out_shape=jax.ShapeDtypeStruct((128, D), bf16),
        in_specs=[vmem] * 10 + [hbm] * 12,
        out_specs=vmem,
        scratch_shapes=[
            pltpu.VMEM((128, 512), bf16),
            pltpu.VMEM((512, 2048), bf16),
            pltpu.VMEM((128, 1536), bf16),
            pltpu.VMEM((32, 128), f32),
            pltpu.VMEM((128, D), bf16),
            pltpu.VMEM((1024, D), bf16),
            pltpu.VMEM((D, 512), bf16),
            pltpu.VMEM((D, 512), bf16),
            pltpu.VMEM((512, D), bf16),
            pltpu.VMEM((D, 512), bf16),
            pltpu.VMEM((D, 512), bf16),
            pltpu.VMEM((512, D), bf16),
            pltpu.VMEM((1536, 128), bf16),
            pltpu.VMEM((16, 256, 128), bf16),
            pltpu.VMEM((16, 256, 128), bf16),
            pltpu.VMEM((2048, 256), bf16),
            pltpu.VMEM((256, 2048), bf16),
            pltpu.VMEM((128, 2048), bf16),
            pltpu.VMEM((2048, 256), f32),
            pltpu.VMEM((16, 64, 128), bf16),
            pltpu.VMEM((16, 64, 128), bf16),
            pltpu.VMEM((128, D), bf16),
            pltpu.VMEM((TOP_K, 128), jnp.int32),
            pltpu.VMEM((128, TOP_K), jnp.int32),
            pltpu.VMEM((128, TOP_K), f32),
            blocks, blocks, blocks, blocks,
            pltpu.VMEM((GROUP_ROWS * TILES, 128), f32),
            pltpu.VMEM((GROUP_ROWS, D), bf16),
            pltpu.VMEM((128, D), f32),
            pltpu.SemaphoreType.DMA((12,)),
            pltpu.SemaphoreType.DMA,
            pltpu.SemaphoreType.DMA,
            pltpu.SemaphoreType.DMA,
            pltpu.SemaphoreType.DMA,
            pltpu.SemaphoreType.DMA,
            pltpu.SemaphoreType.DMA((GROUPS,)),
            pltpu.SemaphoreType.DMA,
            pltpu.SemaphoreType.DMA((GROUPS,)),
        ],
        compiler_params=pltpu.CompilerParams(
            collective_id=1, has_side_effects=True, vmem_limit_bytes=58 * 2**20
        ),
    )(
        ids, ids.T, route_weights[0], keys_rope[0], latent_norm_gain[None], attn_gain[None],
        norm1_gain[None], norm1_bias[None], norm2_gain[None], norm2_bias[None],
        key_value_latent[0], latent_up_weight, queries[0], tables, hidden_in[0],
        out_proj, gate_proj, up_proj, down_proj, shared_gate, shared_up, shared_down,
    )
    return result[None]


def solution(mesh):
    in_specs = (
        P("dp", "sp", None),
        P("dp", "sp", None),
        P("dp", "sp", None),
        P("dp", "sp", None),
        P(),
        P(),
        P(),
        P(),
        P(),
        P(),
        P("dp", "sp", None),
        P("dp", "sp", None),
        P(("sp", "dp"), None, None),
        P(("sp", "dp"), None, None),
        P(("sp", "dp"), None, None),
        P(),
        P(),
        P(),
        P(),
        P(),
    )
    out_specs = P("dp", "sp", None)
    return jax.shard_map(
        per_device, mesh=mesh, in_specs=in_specs, out_specs=out_specs, check_vma=False
    )
```

```python
import math

import jax
import jax.numpy as jnp
import numpy as np
from jax import lax
from jax.experimental import pallas as pl
from jax.experimental.pallas import tpu as pltpu
from jax.sharding import PartitionSpec as P

D = 2048
ATTENTION_HEADS = 16
PLAIN_HEAD_WIDTH = 64
QK_ROPE = 32
VALUE_HEAD_WIDTH = 64
TOP_K = 4


ALPHA = 2.0**0.25
ROUTED = 2.5
THETA = 10000.0


def rms_scaled(values, scaling):
    widened = values.astype(jnp.float32)
    return (
        widened * lax.rsqrt(jnp.mean(widened * widened, axis=-1, keepdims=True) + 1e-06) * scaling
    )


def layer_norm(values, scaling, bias_add):
    centre = values - jnp.mean(values, axis=-1, keepdims=True)
    spread = jnp.mean(centre * centre, axis=-1, keepdims=True)
    return centre * lax.rsqrt(spread + 1e-05) * scaling + bias_add


def rotation_tables(devices, rows):
    frequency = np.power(THETA, -np.arange(0, QK_ROPE, 2) / QK_ROPE).astype(np.float32)
    positions = np.arange(devices * rows, dtype=np.float32).reshape(devices, 1, rows)
    angles = (positions * frequency[None, :, None]).astype(np.float64)
    return np.concatenate([np.cos(angles), np.sin(angles)], axis=1).astype(np.float32)


MESH = pl.DeviceIdType.MESH
GROUPS = 8
PER_GROUP = 16
SLOTS = 6
GROUP_ROWS = PER_GROUP * SLOTS
TILES = D // 128


def position_of(sp, dp):
    return sp // 4, sp % 4, dp // 2, dp % 2


def step_of(k):
    dc, dy, dx = (k // 16) % 2, (k // 4) % 4, k % 4
    return (k // 32 + 8 - dx - dy) % 4, dy, dx, dc


def peer_at(here, k):
    z, y = here[:2]
    dy = k % 4
    return (z + (k // 4 + 4 - dy)) % 4 * 4 + (y + dy) % 4


def device_at(here, k, sign):
    z, y, x, c = here
    dz, dy, dx, dc = step_of(k)
    z, y = (z + 4 + sign * dz) % 4, (y + 4 + sign * dy) % 4
    x, c = (x + 4 + sign * dx) % 4, (c + dc) % 2
    return (z * 4 + y, x * 2 + c)


def order_of(expert_ids, here):
    z, y, x, c = here
    ez, ey, ex, ec = expert_ids // 32, (expert_ids // 8) % 4, (expert_ids // 2) % 4, expert_ids % 2
    dz, dy, dx, dc = (ez - z) & 3, (ey - y) & 3, (ex - x) & 3, (ec + c) & 1
    return (((dz + dy + dx) & 3) * 2 + dc) * 16 + dy * 4 + dx


def iota(shape, dim):
    return lax.broadcasted_iota(jnp.int32, shape, dim)


def layer_kernel(
    ids_t_hbm, weights_t_hbm, rope_t_hbm, latent_gain_hbm, attn_gain_hbm,
    gain1_hbm, bias1_hbm, gain2_hbm, bias2_hbm,
    latent_hbm, latent_up_hbm, queries_hbm, tables_hbm, hidden_hbm,
    out_proj_hbm, gate_hbm, up_hbm, down_hbm, sgate_hbm, sup_hbm, sdown_hbm,
    out_ref,
    ids_t_ref, weights_t_ref, rope_t_ref, latent_gain_ref, attn_gain_ref,
    gain1_ref, bias1_ref, gain2_ref, bias2_ref,
    latent, latent_up, queries, tables, hidden,
    out_proj, gate, up, down, sgate, sup, sdown,
    turned, message, letters, keys, asked, values_t, scores, heads_out, heads_in,
    first, places_t, places, gates, send, arrived, made, returned, flat, rows, total,
    load_sem, msg_sem, letter_sem, value_sem, head_sem, heads_sem,
    send_sem, recv_sem, back_sem, ret_sem,
):
    sp, dp = lax.axis_index("sp"), lax.axis_index("dp")
    here = position_of(sp, dp)
    loads = [
        pltpu.make_async_copy(src, dst, load_sem.at[i])
        for i, (src, dst) in enumerate(
            (
                (latent_hbm, latent), (latent_up_hbm, latent_up), (queries_hbm, queries),
                (tables_hbm.at[sp], tables), (hidden_hbm, hidden), (out_proj_hbm, out_proj),
                (sgate_hbm, sgate), (sup_hbm, sup), (sdown_hbm, sdown),
                (gate_hbm.at[0], gate), (up_hbm.at[0], up), (down_hbm.at[0], down),
                (latent_gain_hbm, latent_gain_ref), (rope_t_hbm, rope_t_ref),
                (ids_t_hbm, ids_t_ref), (weights_t_hbm, weights_t_ref),
                (attn_gain_hbm, attn_gain_ref), (gain1_hbm, gain1_ref), (bias1_hbm, bias1_ref),
                (gain2_hbm, gain2_ref), (bias2_hbm, bias2_ref),
            )
        )
    ]
    for i in (3, 13, 2, 0, 12, 1):
        loads[i].start()
    barrier = pltpu.get_barrier_semaphore()

    def greet(k, carry):
        pl.semaphore_signal(barrier, inc=1, device_id=device_at(here, k, 1), device_id_type=MESH)
        return carry

    lax.fori_loop(1, 128, greet, 0)

    loads[3].wait()
    loads[13].wait()
    cosine, sine = tables[0:16, :], tables[16:32, :]

    def turn(both):
        a, b = both[0:16].astype(jnp.float32), both[16:32].astype(jnp.float32)
        return jnp.concatenate([a * cosine - b * sine, b * cosine + a * sine], axis=0).astype(
            jnp.bfloat16
        )

    rope_t = turn(rope_t_ref[...])
    loads[2].wait()
    for tile in range(12):
        turned[tile * 128 : tile * 128 + 128, :] = queries[:, tile * 128 : tile * 128 + 128].T
    for head in range(16):
        block = turned[head * 96 : head * 96 + 96, :]
        message[head, 0:64, :] = block[0:64]
        message[head, 64:96, :] = turn(block[64:96])
        message[head, 96:128, :] = rope_t
    loads[0].wait()
    loads[12].wait()
    normed = rms_scaled(latent[...], latent_gain_ref[...]).astype(jnp.bfloat16)
    loads[1].wait()
    keys_values = jnp.dot(normed, latent_up[...], preferred_element_type=jnp.float32).astype(
        jnp.bfloat16
    )
    for head in range(16):
        message[head, 128:256, :] = keys_values[:, head * 128 : head * 128 + 128].T
    pl.semaphore_wait(barrier, 127)

    def deliver(rows, sem):
        def one(k, carry):
            peer = peer_at(here, k)
            pltpu.make_async_remote_copy(
                message.at[peer, rows], letters.at[sp, rows], msg_sem, sem,
                device_id=(peer, dp), device_id_type=MESH,
            ).start()
            return carry

        lax.fori_loop(1, 16, one, 0)

    keys_part, values_part = pl.ds(0, 192), pl.ds(192, 64)
    deliver(keys_part, letter_sem)
    deliver(values_part, value_sem)
    letters[sp] = message[sp]
    for i in (14, 15, 4, 5, 16, 17, 18, 6, 7, 8, 9, 10, 11, 19, 20):
        loads[i].start()

    loads[14].wait()
    loads[15].wait()
    ids_t = ids_t_ref[...]
    named_t = jnp.zeros((128, 128), jnp.bool_)
    for col in range(TOP_K):
        named_t = named_t | (iota((128, 128), 0) == ids_t[col : col + 1, :])
    before = (iota((128, 128), 0) < iota((128, 128), 1)).astype(jnp.bfloat16)
    count_t = jnp.dot(named_t.astype(jnp.bfloat16), before, preferred_element_type=jnp.float32)
    order_t = order_of(ids_t, here)
    for col in range(TOP_K):
        slot = jnp.sum(
            jnp.where(iota((128, 128), 0) == ids_t[col : col + 1, :], count_t, 0.0),
            axis=0, keepdims=True,
        )
        places_t[col : col + 1, :] = order_t[col : col + 1, :] * SLOTS + slot.astype(jnp.int32)
    def upright(short):
        filler = jnp.zeros((128 - TOP_K, 128), short.dtype)
        return jnp.concatenate([short, filler], axis=0).T[:, 0:TOP_K]

    places[...] = upright(places_t[...].astype(jnp.float32)).astype(jnp.int32)
    weights = weights_t_ref[...]
    gates[...] = upright(weights / jnp.sum(weights, axis=0, keepdims=True) * ROUTED)

    asked[...] = jnp.zeros_like(asked)
    fifteen = message.at[pl.ds(0, 15)]
    some = message.at[pl.ds(0, 15), keys_part]
    pltpu.make_async_copy(some, some, letter_sem).wait()
    for block in range(16):
        span = slice(block * 128, block * 128 + 128)
        top, plain = letters[block, 0:128, :], letters[block, 128:192, :]
        keys[span, 0:128] = top.T
        keys[span, 128:192] = plain.T
        asked[96:128, span] = top[64:96]
        asked[128:192, span] = top[0:64]

    factor = math.log2(math.e) / math.sqrt(PLAIN_HEAD_WIDTH + QK_ROPE)

    def place_of(index, other):
        return index * (index + 1) // 2 + other

    def score(index):
        asking = asked[:, index * 256 : index * 256 + 256]
        peak = None
        for other in range(index + 1):
            span = slice(other * 256, other * 256 + 256)
            part = jnp.dot(keys[span, :], asking, preferred_element_type=jnp.float32)
            if other == index:
                part = jnp.where(iota((256, 256), 0) <= iota((256, 256), 1), part, -jnp.inf)
            scores[place_of(index, other)] = part
            high = jnp.max(part, axis=0, keepdims=True)
            peak = high if peak is None else jnp.maximum(peak, high)
        return peak * factor

    def attend(index, peak):
        weight, mixed = 0.0, 0.0
        for other in range(index + 1):
            part = jnp.exp2(scores[place_of(index, other)] * factor - peak)
            weight = weight + jnp.sum(part, axis=0, keepdims=True)
            mixed = mixed + jnp.dot(
                values_t[:, other * 256 : other * 256 + 256], part.astype(jnp.bfloat16),
                preferred_element_type=jnp.float32,
            )
        mixed = (mixed / weight).astype(jnp.bfloat16)
        heads_out[2 * index] = mixed[:, 0:128]
        heads_out[2 * index + 1] = mixed[:, 128:256]

    def give_back(base, count):
        def give(k, carry):
            peer = base + (sp + k) % count

            @pl.when(peer != sp)
            def _():
                pltpu.make_async_remote_copy(
                    heads_out.at[peer], heads_in.at[sp], head_sem, heads_sem,
                    device_id=(peer, dp), device_id_type=MESH,
                ).start()

            return carry

        lax.fori_loop(0, count, give, 0)

    peaks = [score(index) for index in range(8)]
    some = message.at[pl.ds(0, 15), values_part]
    pltpu.make_async_copy(some, some, value_sem).wait()
    for block in range(16):
        values_t[:, block * 128 : block * 128 + 128] = letters[block, 192:256, :]
    for index in range(8):
        attend(index, peaks[index])
        if index in (3, 5, 7):
            give_back(*{3: (0, 8), 5: (8, 4), 7: (12, 4)}[index])
    heads_in[sp] = heads_out[sp]
    for load in loads[4:6] + loads[16:21]:
        load.wait()
    arrivals = heads_out.at[pl.ds(0, 15)]
    pltpu.make_async_copy(arrivals, arrivals, heads_sem).wait()
    attended = heads_in[...].reshape(1024, 128).T
    attn_normed = rms_scaled(attended, attn_gain_ref[...]).astype(jnp.bfloat16)
    mixed = jnp.dot(attn_normed, out_proj[...], preferred_element_type=jnp.float32)
    first[...] = layer_norm(
        ALPHA * hidden[...].astype(jnp.float32) + mixed, gain1_ref[...], bias1_ref[...]
    ).astype(jnp.bfloat16)

    def pack(group, source, target):
        for tile in range(TILES):
            flat[pl.ds(tile, GROUP_ROWS, stride=TILES), :] = source[:, tile * 128 : tile * 128 + 128]
        target[pl.ds(group * PER_GROUP, PER_GROUP)] = (
            flat[...].astype(jnp.bfloat16).reshape(PER_GROUP, SLOTS * TILES, 128)
        )

    def unpack(group, source):
        flat[...] = (
            source[pl.ds(group * PER_GROUP, PER_GROUP)]
            .reshape(GROUP_ROWS * TILES, 128)
            .astype(jnp.float32)
        )
        for tile in range(TILES):
            rows[:, tile * 128 : tile * 128 + 128] = flat[
                pl.ds(tile, GROUP_ROWS, stride=TILES), :
            ].astype(jnp.bfloat16)

    def dispatch(k, carry):
        pltpu.make_async_remote_copy(
            send.at[k], arrived.at[k], send_sem, recv_sem.at[k // PER_GROUP],
            device_id=device_at(here, k, 1), device_id_type=MESH,
        ).start()
        return carry

    def reply(k, carry):
        pltpu.make_async_remote_copy(
            made.at[k], returned.at[k], back_sem, ret_sem.at[k // PER_GROUP],
            device_id=device_at(here, k, -1), device_id_type=MESH,
        ).start()
        return carry

    def wait_blocks(group, buffer, sem):
        @pl.when(group == 0)
        def _():
            block = buffer.at[pl.ds(0, PER_GROUP - 1)]
            pltpu.make_async_copy(block, block, sem.at[group]).wait()

        @pl.when(group > 0)
        def _():
            block = buffer.at[pl.ds(0, PER_GROUP)]
            pltpu.make_async_copy(block, block, sem.at[group]).wait()

    def load_group(group, carry):
        picks = iota((GROUP_ROWS, 128), 0) + group * GROUP_ROWS
        chosen = jnp.zeros((GROUP_ROWS, 128), jnp.bool_)
        for col in range(TOP_K):
            chosen = chosen | (picks == places_t[col : col + 1, :])
        out = jnp.dot(
            chosen.astype(jnp.bfloat16), first[...], preferred_element_type=jnp.float32
        )
        pack(group, out, send)

        lax.fori_loop(jnp.maximum(group * PER_GROUP, 1), (group + 1) * PER_GROUP, dispatch, 0)
        return carry

    lax.fori_loop(0, GROUPS, load_group, 0)
    arrived[0] = send[0]

    for load in loads[6:9]:
        load.wait()
    tokens = first[...]
    gated = jnp.dot(tokens, sgate[...], preferred_element_type=jnp.float32)
    lifted = jnp.dot(tokens, sup[...], preferred_element_type=jnp.float32)
    inner = (gated / (1.0 + jnp.exp(-gated)) * lifted).astype(jnp.bfloat16)
    total[...] = ALPHA * tokens.astype(jnp.float32) + jnp.dot(
        inner, sdown[...], preferred_element_type=jnp.float32
    )
    for load in loads[9:12]:
        load.wait()

    def expert_group(group, carry):
        wait_blocks(group, arrived, recv_sem)
        unpack(group, arrived)
        tokens = rows[...]
        gated = jnp.dot(tokens, gate[...], preferred_element_type=jnp.float32)
        lifted = jnp.dot(tokens, up[...], preferred_element_type=jnp.float32)
        inner = (gated / (1.0 + jnp.exp(-gated)) * lifted).astype(jnp.bfloat16)
        out = jnp.dot(inner, down[...], preferred_element_type=jnp.float32)
        pack(group, out, made)
        lax.fori_loop(jnp.maximum(group * PER_GROUP, 1), (group + 1) * PER_GROUP, reply, 0)
        return carry

    lax.fori_loop(0, GROUPS, expert_group, 0)
    returned[0] = made[0]

    def combine_group(group, carry):
        wait_blocks(group, returned, ret_sem)
        unpack(group, returned)
        picks = iota((128, GROUP_ROWS), 1) + group * GROUP_ROWS
        share = jnp.zeros((128, GROUP_ROWS), jnp.float32)
        for col in range(TOP_K):
            share = share + jnp.where(
                picks == places[:, col : col + 1], gates[:, col : col + 1], 0.0
            )
        high = share.astype(jnp.bfloat16)
        low = (share - high.astype(jnp.float32)).astype(jnp.bfloat16)
        tokens = rows[...]
        total[...] += jnp.dot(high, tokens, preferred_element_type=jnp.float32) + jnp.dot(
            low, tokens, preferred_element_type=jnp.float32
        )
        return carry

    lax.fori_loop(0, GROUPS, combine_group, 0)
    out_ref[...] = layer_norm(total[...], gain2_ref[...], bias2_ref[...]).astype(jnp.bfloat16)
    sent = send.at[pl.ds(0, 127)]
    pltpu.make_async_copy(sent, sent, send_sem).wait()
    pltpu.make_async_copy(sent, sent, back_sem).wait()
    pltpu.make_async_copy(fifteen, fifteen, msg_sem).wait()
    pltpu.make_async_copy(arrivals, arrivals, head_sem).wait()


def per_device(
    hidden_in, queries, key_value_latent, keys_rope, latent_norm_gain, latent_up_weight,
    attn_gain, out_proj, norm1_gain, norm1_bias, expert_ids, route_weights,
    gate_proj, up_proj, down_proj, shared_gate, shared_up, shared_down, norm2_gain, norm2_bias,
):
    bf16, f32 = jnp.bfloat16, jnp.float32
    vmem = pl.BlockSpec(memory_space=pltpu.VMEM)
    hbm = pl.BlockSpec(memory_space=pltpu.HBM)
    blocks = pltpu.VMEM((GROUPS * PER_GROUP, SLOTS * TILES, 128), bf16)
    tables = jnp.asarray(rotation_tables(16, 128))
    layer = pl.pallas_call(
        layer_kernel,
        out_shape=jax.ShapeDtypeStruct((128, D), bf16),
        in_specs=[hbm] * 21,
        out_specs=vmem,
        scratch_shapes=[
            pltpu.VMEM((TOP_K, 128), jnp.int32),
            pltpu.VMEM((TOP_K, 128), f32),
            pltpu.VMEM((QK_ROPE, 128), bf16),
            pltpu.VMEM((1, 512), f32),
            pltpu.VMEM((1, 1024), f32),
            pltpu.VMEM((1, D), f32),
            pltpu.VMEM((1, D), f32),
            pltpu.VMEM((1, D), f32),
            pltpu.VMEM((1, D), f32),
            pltpu.VMEM((128, 512), bf16),
            pltpu.VMEM((512, 2048), bf16),
            pltpu.VMEM((128, 1536), bf16),
            pltpu.VMEM((32, 128), f32),
            pltpu.VMEM((128, D), bf16),
            pltpu.VMEM((1024, D), bf16),
            pltpu.VMEM((D, 512), bf16),
            pltpu.VMEM((D, 512), bf16),
            pltpu.VMEM((512, D), bf16),
            pltpu.VMEM((D, 512), bf16),
            pltpu.VMEM((D, 512), bf16),
            pltpu.VMEM((512, D), bf16),
            pltpu.VMEM((1536, 128), bf16),
            pltpu.VMEM((16, 256, 128), bf16),
            pltpu.VMEM((16, 256, 128), bf16),
            pltpu.VMEM((2048, 192), bf16),
            pltpu.VMEM((192, 2048), bf16),
            pltpu.VMEM((64, 2048), bf16),
            pltpu.VMEM((36, 256, 256), f32),
            pltpu.VMEM((16, 64, 128), bf16),
            pltpu.VMEM((16, 64, 128), bf16),
            pltpu.VMEM((128, D), bf16),
            pltpu.VMEM((TOP_K, 128), jnp.int32),
            pltpu.VMEM((128, TOP_K), jnp.int32),
            pltpu.VMEM((128, TOP_K), f32),
            blocks, blocks, blocks, blocks,
            pltpu.VMEM((GROUP_ROWS * TILES, 128), f32),
            pltpu.VMEM((GROUP_ROWS, D), bf16),
            pltpu.VMEM((128, D), f32),
            pltpu.SemaphoreType.DMA((21,)),
            pltpu.SemaphoreType.DMA,
            pltpu.SemaphoreType.DMA,
            pltpu.SemaphoreType.DMA,
            pltpu.SemaphoreType.DMA,
            pltpu.SemaphoreType.DMA,
            pltpu.SemaphoreType.DMA,
            pltpu.SemaphoreType.DMA((GROUPS,)),
            pltpu.SemaphoreType.DMA,
            pltpu.SemaphoreType.DMA((GROUPS,)),
        ],
        compiler_params=pltpu.CompilerParams(
            collective_id=1, has_side_effects=True, vmem_limit_bytes=52 * 2**20
        ),
    )
    operands = (
        expert_ids[0].T, route_weights[0].T, keys_rope[0].T, latent_norm_gain[None],
        attn_gain[None], norm1_gain[None], norm1_bias[None], norm2_gain[None], norm2_bias[None],
        key_value_latent[0], latent_up_weight, queries[0], tables, hidden_in[0],
        out_proj, gate_proj, up_proj, down_proj, shared_gate, shared_up, shared_down,
    )
    result = layer(*(pltpu.with_memory_space_constraint(a, pltpu.HBM) for a in operands))
    return result[None]


def solution(mesh):
    in_specs = (
        P("dp", "sp", None),
        P("dp", "sp", None),
        P("dp", "sp", None),
        P("dp", "sp", None),
        P(),
        P(),
        P(),
        P(),
        P(),
        P(),
        P("dp", "sp", None),
        P("dp", "sp", None),
        P(("sp", "dp"), None, None),
        P(("sp", "dp"), None, None),
        P(("sp", "dp"), None, None),
        P(),
        P(),
        P(),
        P(),
        P(),
    )
    out_specs = P("dp", "sp", None)
    return jax.shard_map(
        per_device, mesh=mesh, in_specs=in_specs, out_specs=out_specs, check_vma=False
    )
```

```python
import math

import jax
import jax.numpy as jnp
import numpy as np
from jax import lax
from jax.experimental import pallas as pl
from jax.experimental.pallas import tpu as pltpu
from jax.sharding import PartitionSpec as P

D = 2048
ATTENTION_HEADS = 16
PLAIN_HEAD_WIDTH = 64
QK_ROPE = 32
VALUE_HEAD_WIDTH = 64
TOP_K = 4


ALPHA = 2.0**0.25
ROUTED = 2.5
THETA = 10000.0


def rms_scaled(values, scaling):
    widened = values.astype(jnp.float32)
    return (
        widened * lax.rsqrt(jnp.mean(widened * widened, axis=-1, keepdims=True) + 1e-06) * scaling
    )


def layer_norm(values, scaling, bias_add):
    centre = values - jnp.mean(values, axis=-1, keepdims=True)
    spread = jnp.mean(centre * centre, axis=-1, keepdims=True)
    return centre * lax.rsqrt(spread + 1e-05) * scaling + bias_add


def rotation_tables(devices, rows):
    frequency = np.power(THETA, -np.arange(0, QK_ROPE, 2) / QK_ROPE).astype(np.float32)
    positions = np.arange(devices * rows, dtype=np.float32).reshape(devices, 1, rows)
    angles = (positions * frequency[None, :, None]).astype(np.float64)
    return np.concatenate([np.cos(angles), np.sin(angles)], axis=1).astype(np.float32)


MESH = pl.DeviceIdType.MESH
GROUPS = 8
PER_GROUP = 16
SLOTS = 6
GROUP_ROWS = PER_GROUP * SLOTS
TILES = D // 128


def position_of(sp, dp):
    return sp // 4, sp % 4, dp // 2, dp % 2


def order_of(expert_ids, here):
    z, y, x, c = here
    ez, ey, ex, ec = expert_ids // 32, (expert_ids // 8) % 4, (expert_ids // 2) % 4, expert_ids % 2
    dz, dy, dx, dc = (ez - z) & 3, (ey - y) & 3, (ex - x) & 3, (ec + c) & 1
    return (((dz + dy + dx) & 3) * 2 + dc) * 16 + dy * 4 + dx


def iota(shape, dim):
    return lax.broadcasted_iota(jnp.int32, shape, dim)


def layer_kernel(
    ids_t_hbm, weights_t_hbm, rope_t_hbm, latent_gain_hbm, attn_gain_hbm,
    gain1_hbm, bias1_hbm, gain2_hbm, bias2_hbm,
    latent_hbm, latent_up_hbm, queries_hbm, tables_hbm, hidden_hbm,
    out_proj_hbm, gate_hbm, up_hbm, down_hbm, sgate_hbm, sup_hbm, sdown_hbm,
    out_ref,
    ids_t_ref, weights_t_ref, rope_t_ref, latent_gain_ref, attn_gain_ref,
    gain1_ref, bias1_ref, gain2_ref, bias2_ref,
    latent, latent_up, queries, tables, hidden,
    out_proj, gate, up, down, sgate, sup, sdown,
    turned, message, letters, keys, asked, values_t, scores, probs, heads_out, heads_in,
    first, places_t, places, gates, send, arrived, made, returned, flat, rows, total,
    load_sem, msg_sem, letter_sem, value_sem, head_sem, heads_sem,
    send_sem, recv_sem, back_sem, ret_sem,
):
    sp, dp = lax.axis_index("sp"), lax.axis_index("dp")
    here = position_of(sp, dp)
    loads = [
        pltpu.make_async_copy(src, dst, load_sem.at[i])
        for i, (src, dst) in enumerate(
            (
                (latent_hbm, latent), (latent_up_hbm, latent_up), (queries_hbm, queries),
                (tables_hbm.at[sp], tables), (hidden_hbm, hidden), (out_proj_hbm, out_proj),
                (sgate_hbm, sgate), (sup_hbm, sup), (sdown_hbm, sdown),
                (gate_hbm.at[0], gate), (up_hbm.at[0], up), (down_hbm.at[0], down),
                (latent_gain_hbm, latent_gain_ref), (rope_t_hbm, rope_t_ref),
                (ids_t_hbm, ids_t_ref), (weights_t_hbm, weights_t_ref),
                (attn_gain_hbm, attn_gain_ref), (gain1_hbm, gain1_ref), (bias1_hbm, bias1_ref),
                (gain2_hbm, gain2_ref), (bias2_hbm, bias2_ref),
            )
        )
    ]
    for i in (3, 13, 2, 0, 12, 1):
        loads[i].start()
    barrier = pltpu.get_barrier_semaphore()

    columns = [lax.rem(dp + j, 8) for j in range(8)]

    def greet(i, carry):
        row = lax.rem(sp + i, 16)

        def signal(column):
            pl.semaphore_signal(barrier, inc=1, device_id=(row, column), device_id_type=MESH)

        for j in range(1, 8):
            signal(columns[j])

        @pl.when(i > 0)
        def _():
            signal(columns[0])

        return carry

    lax.fori_loop(0, 16, greet, 0)
    z, y, x, c = here
    z_plus, y_plus, x_plus = ([lax.rem(v + j, 4) for j in range(4)] for v in (z, y, x))
    y_minus, x_minus = ([lax.rem(v + 4 - j, 4) for j in range(4)] for v in (y, x))

    loads[3].wait()
    loads[13].wait()
    cosine, sine = tables[0:16, :], tables[16:32, :]

    def turn(both):
        a, b = both[0:16].astype(jnp.float32), both[16:32].astype(jnp.float32)
        return jnp.concatenate([a * cosine - b * sine, b * cosine + a * sine], axis=0).astype(
            jnp.bfloat16
        )

    rope_t = turn(rope_t_ref[...])
    loads[2].wait()
    for tile in range(12):
        turned[tile * 128 : tile * 128 + 128, :] = queries[:, tile * 128 : tile * 128 + 128].T
    for head in range(16):
        block = turned[head * 96 : head * 96 + 96, :]
        message[head, 0:64, :] = block[0:64]
        message[head, 64:96, :] = turn(block[64:96])
        message[head, 96:128, :] = rope_t
    loads[0].wait()
    loads[12].wait()
    normed = rms_scaled(latent[...], latent_gain_ref[...]).astype(jnp.bfloat16)
    loads[1].wait()
    keys_values = jnp.dot(normed, latent_up[...], preferred_element_type=jnp.float32).astype(
        jnp.bfloat16
    )
    for head in range(16):
        message[head, 128:256, :] = keys_values[:, head * 128 : head * 128 + 128].T
    pl.semaphore_wait(barrier, 127)

    def deliver(rows, sem):
        for k in range(1, 16):
            peer = z_plus[(k // 4 - k) % 4] * 4 + y_plus[k % 4]
            pltpu.make_async_remote_copy(
                message.at[peer, rows], letters.at[sp, rows], msg_sem, sem,
                device_id=(peer, dp), device_id_type=MESH,
            ).start()

    keys_part, values_part = pl.ds(0, 192), pl.ds(192, 64)
    deliver(keys_part, letter_sem)
    deliver(values_part, value_sem)
    letters[sp] = message[sp]
    for i in (14, 15, 4, 5, 16, 17, 18, 6, 7, 8, 9, 10, 11, 19, 20):
        loads[i].start()

    loads[14].wait()
    loads[15].wait()
    ids_t = ids_t_ref[...]
    named_t = jnp.zeros((128, 128), jnp.bool_)
    for col in range(TOP_K):
        named_t = named_t | (iota((128, 128), 0) == ids_t[col : col + 1, :])
    before = (iota((128, 128), 0) < iota((128, 128), 1)).astype(jnp.bfloat16)
    count_t = jnp.dot(named_t.astype(jnp.bfloat16), before, preferred_element_type=jnp.float32)
    order_t = order_of(ids_t, here)
    for col in range(TOP_K):
        slot = jnp.sum(
            jnp.where(iota((128, 128), 0) == ids_t[col : col + 1, :], count_t, 0.0),
            axis=0, keepdims=True,
        )
        places_t[col : col + 1, :] = order_t[col : col + 1, :] * SLOTS + slot.astype(jnp.int32)
    def upright(short):
        filler = jnp.zeros((128 - TOP_K, 128), short.dtype)
        return jnp.concatenate([short, filler], axis=0).T[:, 0:TOP_K]

    places[...] = upright(places_t[...].astype(jnp.float32)).astype(jnp.int32)
    weights = weights_t_ref[...]
    gates[...] = upright(weights / jnp.sum(weights, axis=0, keepdims=True) * ROUTED)

    asked[...] = jnp.zeros_like(asked)
    fifteen = message.at[pl.ds(0, 15)]
    some = message.at[pl.ds(0, 15), keys_part]
    pltpu.make_async_copy(some, some, letter_sem).wait()
    for block in range(16):
        span = slice(block * 128, block * 128 + 128)
        top, plain = letters[block, 0:128, :], letters[block, 128:192, :]
        keys[span, 0:128] = top.T
        keys[span, 128:192] = plain.T
        asked[96:128, span] = top[64:96]
        asked[128:192, span] = top[0:64]

    factor = math.log2(math.e) / math.sqrt(PLAIN_HEAD_WIDTH + QK_ROPE)

    def place_of(index, other):
        return index * (index + 1) // 2 + other

    def weigh(index):
        asking = asked[:, index * 256 : index * 256 + 256]
        peak, weight = None, 0.0
        for other in range(index + 1):
            part = jnp.dot(
                keys[other * 256 : other * 256 + 256, :], asking,
                preferred_element_type=jnp.float32,
            )
            if other == index:
                part = jnp.where(iota((256, 256), 0) <= iota((256, 256), 1), part, -jnp.inf)
            scores[index % 2, other] = part
            high = jnp.max(part, axis=0, keepdims=True)
            peak = high if peak is None else jnp.maximum(peak, high)
        peak = peak * factor
        for other in range(index + 1):
            part = jnp.exp2(scores[index % 2, other] * factor - peak)
            weight = weight + jnp.sum(part, axis=0, keepdims=True)
            probs[place_of(index, other)] = part.astype(jnp.bfloat16)
        return weight

    def attend(index, weight):
        mixed = 0.0
        for other in range(index + 1):
            mixed = mixed + jnp.dot(
                values_t[:, other * 256 : other * 256 + 256], probs[place_of(index, other)],
                preferred_element_type=jnp.float32,
            )
        mixed = (mixed / weight).astype(jnp.bfloat16)
        heads_out[2 * index] = mixed[:, 0:128]
        heads_out[2 * index + 1] = mixed[:, 128:256]

    def give_back(base, count):
        def give(k, carry):
            peer = base + (sp + k) % count

            @pl.when(peer != sp)
            def _():
                pltpu.make_async_remote_copy(
                    heads_out.at[peer], heads_in.at[sp], head_sem, heads_sem,
                    device_id=(peer, dp), device_id_type=MESH,
                ).start()

            return carry

        lax.fori_loop(0, count, give, 0)

    sums = [weigh(index) for index in range(8)]
    some = message.at[pl.ds(0, 15), values_part]
    pltpu.make_async_copy(some, some, value_sem).wait()
    for block in range(16):
        values_t[:, block * 128 : block * 128 + 128] = letters[block, 192:256, :]
    for index in range(8):
        attend(index, sums[index])
        if index in (3, 5, 7):
            give_back(*{3: (0, 8), 5: (8, 4), 7: (12, 4)}[index])
    heads_in[sp] = heads_out[sp]
    for load in loads[4:6] + loads[16:21]:
        load.wait()
    arrivals = heads_out.at[pl.ds(0, 15)]
    pltpu.make_async_copy(arrivals, arrivals, heads_sem).wait()
    attended = heads_in[...].reshape(1024, 128).T
    attn_normed = rms_scaled(attended, attn_gain_ref[...]).astype(jnp.bfloat16)
    mixed = jnp.dot(attn_normed, out_proj[...], preferred_element_type=jnp.float32)
    first[...] = layer_norm(
        ALPHA * hidden[...].astype(jnp.float32) + mixed, gain1_ref[...], bias1_ref[...]
    ).astype(jnp.bfloat16)

    def pack(group, source, target):
        for tile in range(TILES):
            flat[pl.ds(tile, GROUP_ROWS, stride=TILES), :] = source[:, tile * 128 : tile * 128 + 128]
        target[pl.ds(group * PER_GROUP, PER_GROUP)] = (
            flat[...].astype(jnp.bfloat16).reshape(PER_GROUP, SLOTS * TILES, 128)
        )

    def unpack(group, source):
        flat[...] = (
            source[pl.ds(group * PER_GROUP, PER_GROUP)]
            .reshape(GROUP_ROWS * TILES, 128)
            .astype(jnp.float32)
        )
        for tile in range(TILES):
            rows[:, tile * 128 : tile * 128 + 128] = flat[
                pl.ds(tile, GROUP_ROWS, stride=TILES), :
            ].astype(jnp.bfloat16)

    def post(group, source, target, out_sem, in_sem, sign):
        turn_z, core = z + 8 + sign * (group // 2), lax.rem(c + group % 2, 2)
        z_of = [lax.rem(turn_z - sign * j, 4) for j in range(4)]
        y_of, x_of = (y_plus, x_plus) if sign > 0 else (y_minus, x_minus)
        for i in range(PER_GROUP):
            dy, dx = i // 4, i % 4

            def start(i=i, dy=dy, dx=dx):
                k = group * PER_GROUP + i
                peer = (z_of[(dy + dx) % 4] * 4 + y_of[dy], x_of[dx] * 2 + core)
                pltpu.make_async_remote_copy(
                    source.at[k], target.at[k], out_sem, in_sem.at[group],
                    device_id=peer, device_id_type=MESH,
                ).start()

            if i == 0:
                pl.when(group > 0)(start)
            else:
                start()

    def wait_blocks(group, buffer, sem):
        @pl.when(group == 0)
        def _():
            block = buffer.at[pl.ds(0, PER_GROUP - 1)]
            pltpu.make_async_copy(block, block, sem.at[group]).wait()

        @pl.when(group > 0)
        def _():
            block = buffer.at[pl.ds(0, PER_GROUP)]
            pltpu.make_async_copy(block, block, sem.at[group]).wait()

    def load_group(group, carry):
        picks = iota((GROUP_ROWS, 128), 0) + group * GROUP_ROWS
        chosen = jnp.zeros((GROUP_ROWS, 128), jnp.bool_)
        for col in range(TOP_K):
            chosen = chosen | (picks == places_t[col : col + 1, :])
        out = jnp.dot(
            chosen.astype(jnp.bfloat16), first[...], preferred_element_type=jnp.float32
        )
        pack(group, out, send)

        post(group, send, arrived, send_sem, recv_sem, 1)
        return carry

    lax.fori_loop(0, GROUPS, load_group, 0)
    arrived[0] = send[0]

    for load in loads[6:9]:
        load.wait()
    tokens = first[...]
    gated = jnp.dot(tokens, sgate[...], preferred_element_type=jnp.float32)
    lifted = jnp.dot(tokens, sup[...], preferred_element_type=jnp.float32)
    inner = (gated / (1.0 + jnp.exp(-gated)) * lifted).astype(jnp.bfloat16)
    total[...] = ALPHA * tokens.astype(jnp.float32) + jnp.dot(
        inner, sdown[...], preferred_element_type=jnp.float32
    )
    for load in loads[9:12]:
        load.wait()

    def expert_group(group, carry):
        wait_blocks(group, arrived, recv_sem)
        unpack(group, arrived)
        tokens = rows[...]
        gated = jnp.dot(tokens, gate[...], preferred_element_type=jnp.float32)
        lifted = jnp.dot(tokens, up[...], preferred_element_type=jnp.float32)
        inner = (gated / (1.0 + jnp.exp(-gated)) * lifted).astype(jnp.bfloat16)
        out = jnp.dot(inner, down[...], preferred_element_type=jnp.float32)
        pack(group, out, made)
        post(group, made, returned, back_sem, ret_sem, -1)
        return carry

    lax.fori_loop(0, GROUPS, expert_group, 0)
    returned[0] = made[0]

    def combine_group(group, carry):
        wait_blocks(group, returned, ret_sem)
        unpack(group, returned)
        picks = iota((128, GROUP_ROWS), 1) + group * GROUP_ROWS
        share = jnp.zeros((128, GROUP_ROWS), jnp.float32)
        for col in range(TOP_K):
            share = share + jnp.where(
                picks == places[:, col : col + 1], gates[:, col : col + 1], 0.0
            )
        high = share.astype(jnp.bfloat16)
        low = (share - high.astype(jnp.float32)).astype(jnp.bfloat16)
        tokens = rows[...]
        total[...] += jnp.dot(high, tokens, preferred_element_type=jnp.float32) + jnp.dot(
            low, tokens, preferred_element_type=jnp.float32
        )
        return carry

    lax.fori_loop(0, GROUPS, combine_group, 0)
    out_ref[...] = layer_norm(total[...], gain2_ref[...], bias2_ref[...]).astype(jnp.bfloat16)
    sent = send.at[pl.ds(0, 127)]
    pltpu.make_async_copy(sent, sent, send_sem).wait()
    pltpu.make_async_copy(sent, sent, back_sem).wait()
    pltpu.make_async_copy(fifteen, fifteen, msg_sem).wait()
    pltpu.make_async_copy(arrivals, arrivals, head_sem).wait()


def per_device(
    hidden_in, queries, key_value_latent, keys_rope, latent_norm_gain, latent_up_weight,
    attn_gain, out_proj, norm1_gain, norm1_bias, expert_ids, route_weights,
    gate_proj, up_proj, down_proj, shared_gate, shared_up, shared_down, norm2_gain, norm2_bias,
):
    bf16, f32 = jnp.bfloat16, jnp.float32
    vmem = pl.BlockSpec(memory_space=pltpu.VMEM)
    hbm = pl.BlockSpec(memory_space=pltpu.HBM)
    blocks = pltpu.VMEM((GROUPS * PER_GROUP, SLOTS * TILES, 128), bf16)
    tables = jnp.asarray(rotation_tables(16, 128))
    layer = pl.pallas_call(
        layer_kernel,
        out_shape=jax.ShapeDtypeStruct((128, D), bf16),
        in_specs=[hbm] * 21,
        out_specs=vmem,
        scratch_shapes=[
            pltpu.VMEM((TOP_K, 128), jnp.int32),
            pltpu.VMEM((TOP_K, 128), f32),
            pltpu.VMEM((QK_ROPE, 128), bf16),
            pltpu.VMEM((1, 512), f32),
            pltpu.VMEM((1, 1024), f32),
            pltpu.VMEM((1, D), f32),
            pltpu.VMEM((1, D), f32),
            pltpu.VMEM((1, D), f32),
            pltpu.VMEM((1, D), f32),
            pltpu.VMEM((128, 512), bf16),
            pltpu.VMEM((512, 2048), bf16),
            pltpu.VMEM((128, 1536), bf16),
            pltpu.VMEM((32, 128), f32),
            pltpu.VMEM((128, D), bf16),
            pltpu.VMEM((1024, D), bf16),
            pltpu.VMEM((D, 512), bf16),
            pltpu.VMEM((D, 512), bf16),
            pltpu.VMEM((512, D), bf16),
            pltpu.VMEM((D, 512), bf16),
            pltpu.VMEM((D, 512), bf16),
            pltpu.VMEM((512, D), bf16),
            pltpu.VMEM((1536, 128), bf16),
            pltpu.VMEM((16, 256, 128), bf16),
            pltpu.VMEM((16, 256, 128), bf16),
            pltpu.VMEM((2048, 192), bf16),
            pltpu.VMEM((192, 2048), bf16),
            pltpu.VMEM((64, 2048), bf16),
            pltpu.VMEM((2, 8, 256, 256), f32),
            pltpu.VMEM((36, 256, 256), bf16),
            pltpu.VMEM((16, 64, 128), bf16),
            pltpu.VMEM((16, 64, 128), bf16),
            pltpu.VMEM((128, D), bf16),
            pltpu.VMEM((TOP_K, 128), jnp.int32),
            pltpu.VMEM((128, TOP_K), jnp.int32),
            pltpu.VMEM((128, TOP_K), f32),
            blocks, blocks, blocks, blocks,
            pltpu.VMEM((GROUP_ROWS * TILES, 128), f32),
            pltpu.VMEM((GROUP_ROWS, D), bf16),
            pltpu.VMEM((128, D), f32),
            pltpu.SemaphoreType.DMA((21,)),
            pltpu.SemaphoreType.DMA,
            pltpu.SemaphoreType.DMA,
            pltpu.SemaphoreType.DMA,
            pltpu.SemaphoreType.DMA,
            pltpu.SemaphoreType.DMA,
            pltpu.SemaphoreType.DMA,
            pltpu.SemaphoreType.DMA((GROUPS,)),
            pltpu.SemaphoreType.DMA,
            pltpu.SemaphoreType.DMA((GROUPS,)),
        ],
        compiler_params=pltpu.CompilerParams(
            collective_id=1, has_side_effects=True, vmem_limit_bytes=52 * 2**20
        ),
    )
    operands = (
        expert_ids[0].T, route_weights[0].T, keys_rope[0].T, latent_norm_gain[None],
        attn_gain[None], norm1_gain[None], norm1_bias[None], norm2_gain[None], norm2_bias[None],
        key_value_latent[0], latent_up_weight, queries[0], tables, hidden_in[0],
        out_proj, gate_proj, up_proj, down_proj, shared_gate, shared_up, shared_down,
    )
    result = layer(*(pltpu.with_memory_space_constraint(a, pltpu.HBM) for a in operands))
    return result[None]


def solution(mesh):
    in_specs = (
        P("dp", "sp", None),
        P("dp", "sp", None),
        P("dp", "sp", None),
        P("dp", "sp", None),
        P(),
        P(),
        P(),
        P(),
        P(),
        P(),
        P("dp", "sp", None),
        P("dp", "sp", None),
        P(("sp", "dp"), None, None),
        P(("sp", "dp"), None, None),
        P(("sp", "dp"), None, None),
        P(),
        P(),
        P(),
        P(),
        P(),
    )
    out_specs = P("dp", "sp", None)
    return jax.shard_map(
        per_device, mesh=mesh, in_specs=in_specs, out_specs=out_specs, check_vma=False
    )
```

```python
import math

import jax
import jax.numpy as jnp
import numpy as np
from jax import lax
from jax.experimental import pallas as pl
from jax.experimental.pallas import tpu as pltpu
from jax.sharding import PartitionSpec as P

D = 2048
ATTENTION_HEADS = 16
PLAIN_HEAD_WIDTH = 64
QK_ROPE = 32
VALUE_HEAD_WIDTH = 64
TOP_K = 4


ALPHA = 2.0**0.25
ROUTED = 2.5
THETA = 10000.0


def rms_scaled(values, scaling):
    widened = values.astype(jnp.float32)
    return (
        widened * lax.rsqrt(jnp.mean(widened * widened, axis=-1, keepdims=True) + 1e-06) * scaling
    )


def layer_norm(values, scaling, bias_add):
    centre = values - jnp.mean(values, axis=-1, keepdims=True)
    spread = jnp.mean(centre * centre, axis=-1, keepdims=True)
    return centre * lax.rsqrt(spread + 1e-05) * scaling + bias_add


def rotation_tables(devices, rows):
    frequency = np.power(THETA, -np.arange(0, QK_ROPE, 2) / QK_ROPE).astype(np.float32)
    positions = np.arange(devices * rows, dtype=np.float32).reshape(devices, 1, rows)
    angles = (positions * frequency[None, :, None]).astype(np.float64)
    return np.concatenate([np.cos(angles), np.sin(angles)], axis=1).astype(np.float32)


MESH = pl.DeviceIdType.MESH
GROUPS = 8
PER_GROUP = 16
SLOTS = 6
GROUP_ROWS = PER_GROUP * SLOTS
TILES = D // 128


def position_of(sp, dp):
    return sp // 4, sp % 4, dp // 2, dp % 2


def order_of(expert_ids, here):
    z, y, x, c = here
    ez, ey, ex, ec = expert_ids // 32, (expert_ids // 8) % 4, (expert_ids // 2) % 4, expert_ids % 2
    dz, dy, dx, dc = (ez - z) & 3, (ey - y) & 3, (ex - x) & 3, (ec + c) & 1
    return (((dz + dy + dx) & 3) * 2 + dc) * 16 + dy * 4 + dx


def iota(shape, dim):
    return lax.broadcasted_iota(jnp.int32, shape, dim)


def layer_kernel(
    ids_t_hbm, weights_t_hbm, rope_t_hbm, latent_gain_hbm, attn_gain_hbm,
    gain1_hbm, bias1_hbm, gain2_hbm, bias2_hbm,
    latent_hbm, latent_up_hbm, queries_hbm, tables_hbm, hidden_hbm,
    out_proj_hbm, gate_hbm, up_hbm, down_hbm, sgate_hbm, sup_hbm, sdown_hbm,
    out_ref,
    ids_t_ref, weights_t_ref, rope_t_ref, latent_gain_ref, attn_gain_ref,
    gain1_ref, bias1_ref, gain2_ref, bias2_ref,
    latent, latent_up, queries, tables, hidden,
    out_proj, gate, up, down, sgate, sup, sdown,
    turned, message, letters, keys, asked, values_t, scores, probs, heads_out, heads_in,
    first, places_t, places, gates, send, arrived, made, returned, flat, rows, total,
    load_sem, msg_sem, letter_sem, value_sem, head_sem, heads_sem,
    send_sem, recv_sem, back_sem, ret_sem,
):
    sp, dp = lax.axis_index("sp"), lax.axis_index("dp")
    here = position_of(sp, dp)
    loads = [
        pltpu.make_async_copy(src, dst, load_sem.at[i])
        for i, (src, dst) in enumerate(
            (
                (latent_hbm, latent), (latent_up_hbm, latent_up), (queries_hbm, queries),
                (tables_hbm.at[sp], tables), (hidden_hbm, hidden), (out_proj_hbm, out_proj),
                (sgate_hbm, sgate), (sup_hbm, sup), (sdown_hbm, sdown),
                (gate_hbm.at[0], gate), (up_hbm.at[0], up), (down_hbm.at[0], down),
                (latent_gain_hbm, latent_gain_ref), (rope_t_hbm, rope_t_ref),
                (ids_t_hbm, ids_t_ref), (weights_t_hbm, weights_t_ref),
                (attn_gain_hbm, attn_gain_ref), (gain1_hbm, gain1_ref), (bias1_hbm, bias1_ref),
                (gain2_hbm, gain2_ref), (bias2_hbm, bias2_ref),
            )
        )
    ]
    for i in (3, 13, 2, 0, 12, 1):
        loads[i].start()
    barrier = pltpu.get_barrier_semaphore()

    columns = [lax.rem(dp + j, 8) for j in range(8)]

    def greet(i, carry):
        row = lax.rem(sp + i, 16)

        def signal(column):
            pl.semaphore_signal(barrier, inc=1, device_id=(row, column), device_id_type=MESH)

        for j in range(1, 8):
            signal(columns[j])

        @pl.when(i > 0)
        def _():
            signal(columns[0])

        return carry

    lax.fori_loop(0, 16, greet, 0)
    z, y, x, c = here
    z_plus, y_plus, x_plus = ([lax.rem(v + j, 4) for j in range(4)] for v in (z, y, x))
    y_minus, x_minus = ([lax.rem(v + 4 - j, 4) for j in range(4)] for v in (y, x))

    loads[3].wait()
    loads[13].wait()
    cosine, sine = tables[0:16, :], tables[16:32, :]

    def turn(both):
        a, b = both[0:16].astype(jnp.float32), both[16:32].astype(jnp.float32)
        return jnp.concatenate([a * cosine - b * sine, b * cosine + a * sine], axis=0).astype(
            jnp.bfloat16
        )

    rope_t = turn(rope_t_ref[...])
    loads[2].wait()
    for tile in range(12):
        turned[tile * 128 : tile * 128 + 128, :] = queries[:, tile * 128 : tile * 128 + 128].T
    for head in range(16):
        block = turned[head * 96 : head * 96 + 96, :]
        message[head, 0:64, :] = block[0:64]
        message[head, 64:96, :] = turn(block[64:96])
        message[head, 96:128, :] = rope_t
    loads[0].wait()
    loads[12].wait()
    normed = rms_scaled(latent[...], latent_gain_ref[...]).astype(jnp.bfloat16)
    loads[1].wait()
    keys_values = jnp.dot(normed, latent_up[...], preferred_element_type=jnp.float32).astype(
        jnp.bfloat16
    )
    for head in range(16):
        message[head, 128:256, :] = keys_values[:, head * 128 : head * 128 + 128].T
    pl.semaphore_wait(barrier, 127)

    def deliver(rows, sem):
        for k in range(1, 16):
            peer = z_plus[(k // 4 - k) % 4] * 4 + y_plus[k % 4]
            pltpu.make_async_remote_copy(
                message.at[peer, rows], letters.at[sp, rows], msg_sem, sem,
                device_id=(peer, dp), device_id_type=MESH,
            ).start()

    keys_part, values_part = pl.ds(0, 192), pl.ds(192, 64)
    deliver(keys_part, letter_sem)
    deliver(values_part, value_sem)
    letters[sp] = message[sp]
    for i in (14, 15, 4, 5, 16, 17, 18, 6, 7, 8, 9, 10, 11, 19, 20):
        loads[i].start()

    loads[14].wait()
    loads[15].wait()
    ids_t = ids_t_ref[...]
    named_t = jnp.zeros((128, 128), jnp.bool_)
    for col in range(TOP_K):
        named_t = named_t | (iota((128, 128), 0) == ids_t[col : col + 1, :])
    before = (iota((128, 128), 0) < iota((128, 128), 1)).astype(jnp.bfloat16)
    count_t = jnp.dot(named_t.astype(jnp.bfloat16), before, preferred_element_type=jnp.float32)
    order_t = order_of(ids_t, here)
    for col in range(TOP_K):
        slot = jnp.sum(
            jnp.where(iota((128, 128), 0) == ids_t[col : col + 1, :], count_t, 0.0),
            axis=0, keepdims=True,
        )
        places_t[col : col + 1, :] = order_t[col : col + 1, :] * SLOTS + slot.astype(jnp.int32)
    def upright(short):
        filler = jnp.zeros((128 - TOP_K, 128), short.dtype)
        return jnp.concatenate([short, filler], axis=0).T[:, 0:TOP_K]

    places[...] = upright(places_t[...].astype(jnp.float32)).astype(jnp.int32)
    weights = weights_t_ref[...]
    gates[...] = upright(weights / jnp.sum(weights, axis=0, keepdims=True) * ROUTED)

    asked[...] = jnp.zeros_like(asked)
    fifteen = message.at[pl.ds(0, 15)]
    some = message.at[pl.ds(0, 15), keys_part]
    pltpu.make_async_copy(some, some, letter_sem).wait()
    for block in range(16):
        span = slice(block * 128, block * 128 + 128)
        top, plain = letters[block, 0:128, :], letters[block, 128:192, :]
        keys[span, 0:128] = top.T
        keys[span, 128:192] = plain.T
        asked[96:128, span] = top[64:96]
        asked[128:192, span] = top[0:64]

    factor = math.log2(math.e) / math.sqrt(PLAIN_HEAD_WIDTH + QK_ROPE)

    def place_of(index, other):
        return index * (index + 1) // 2 + other

    def weigh(index):
        asking = asked[:, index * 256 : index * 256 + 256]
        peak, weight = None, 0.0
        for other in range(index + 1):
            part = jnp.dot(
                keys[other * 256 : other * 256 + 256, :], asking,
                preferred_element_type=jnp.float32,
            )
            if other == index:
                part = jnp.where(iota((256, 256), 0) <= iota((256, 256), 1), part, -jnp.inf)
            scores[index % 2, other] = part
            high = jnp.max(part, axis=0, keepdims=True)
            peak = high if peak is None else jnp.maximum(peak, high)
        peak = peak * factor
        for other in range(index + 1):
            part = jnp.exp2(scores[index % 2, other] * factor - peak)
            weight = weight + jnp.sum(part, axis=0, keepdims=True)
            probs[place_of(index, other)] = part.astype(jnp.bfloat16)
        return weight

    def attend(index, weight):
        mixed = 0.0
        for other in range(index + 1):
            mixed = mixed + jnp.dot(
                values_t[:, other * 256 : other * 256 + 256], probs[place_of(index, other)],
                preferred_element_type=jnp.float32,
            )
        mixed = (mixed / weight).astype(jnp.bfloat16)
        heads_out[2 * index] = mixed[:, 0:128]
        heads_out[2 * index + 1] = mixed[:, 128:256]

    def give_back(base, count):
        def give(k, carry):
            peer = base + (sp + k) % count

            @pl.when(peer != sp)
            def _():
                pltpu.make_async_remote_copy(
                    heads_out.at[peer], heads_in.at[sp], head_sem, heads_sem,
                    device_id=(peer, dp), device_id_type=MESH,
                ).start()

            return carry

        lax.fori_loop(0, count, give, 0)

    sums = [weigh(index) for index in range(8)]
    some = message.at[pl.ds(0, 15), values_part]
    pltpu.make_async_copy(some, some, value_sem).wait()
    for block in range(16):
        values_t[:, block * 128 : block * 128 + 128] = letters[block, 192:256, :]
    for index in range(8):
        attend(index, sums[index])
        if index in (3, 5, 7):
            give_back(*{3: (0, 8), 5: (8, 4), 7: (12, 4)}[index])
    heads_in[sp] = heads_out[sp]
    for load in loads[4:6] + loads[16:21]:
        load.wait()
    arrivals = heads_out.at[pl.ds(0, 15)]
    pltpu.make_async_copy(arrivals, arrivals, heads_sem).wait()
    attended = heads_in[...].reshape(1024, 128).T
    attn_normed = rms_scaled(attended, attn_gain_ref[...]).astype(jnp.bfloat16)
    mixed = jnp.dot(attn_normed, out_proj[...], preferred_element_type=jnp.float32)
    first[...] = layer_norm(
        ALPHA * hidden[...].astype(jnp.float32) + mixed, gain1_ref[...], bias1_ref[...]
    ).astype(jnp.bfloat16)

    def pack(group, source, target):
        for tile in range(TILES):
            flat[pl.ds(tile, GROUP_ROWS, stride=TILES), :] = source[:, tile * 128 : tile * 128 + 128]
        target[pl.ds(group * PER_GROUP, PER_GROUP)] = (
            flat[...].astype(jnp.bfloat16).reshape(PER_GROUP, SLOTS * TILES, 128)
        )

    def unpack(group, source):
        flat[...] = (
            source[pl.ds(group * PER_GROUP, PER_GROUP)]
            .reshape(GROUP_ROWS * TILES, 128)
            .astype(jnp.float32)
        )
        for tile in range(TILES):
            rows[:, tile * 128 : tile * 128 + 128] = flat[
                pl.ds(tile, GROUP_ROWS, stride=TILES), :
            ].astype(jnp.bfloat16)

    def post(group, source, target, out_sem, in_sem, sign):
        turn_z, core = z + 8 + sign * (group // 2), lax.rem(c + group % 2, 2)
        z_of = [lax.rem(turn_z - sign * j, 4) for j in range(4)]
        y_of, x_of = (y_plus, x_plus) if sign > 0 else (y_minus, x_minus)
        for i in (0, 5, 10, 15, 1, 6, 11, 12, 2, 7, 8, 13, 3, 4, 9, 14):
            dy, dx = i // 4, i % 4

            def start(i=i, dy=dy, dx=dx):
                k = group * PER_GROUP + i
                peer = (z_of[(dy + dx) % 4] * 4 + y_of[dy], x_of[dx] * 2 + core)
                pltpu.make_async_remote_copy(
                    source.at[k], target.at[k], out_sem, in_sem.at[group],
                    device_id=peer, device_id_type=MESH,
                ).start()

            if i == 0:
                pl.when(group > 0)(start)
            else:
                start()

    def wait_blocks(group, buffer, sem):
        @pl.when(group == 0)
        def _():
            block = buffer.at[pl.ds(0, PER_GROUP - 1)]
            pltpu.make_async_copy(block, block, sem.at[group]).wait()

        @pl.when(group > 0)
        def _():
            block = buffer.at[pl.ds(0, PER_GROUP)]
            pltpu.make_async_copy(block, block, sem.at[group]).wait()

    def load_group(group, carry):
        picks = iota((GROUP_ROWS, 128), 0) + group * GROUP_ROWS
        chosen = jnp.zeros((GROUP_ROWS, 128), jnp.bool_)
        for col in range(TOP_K):
            chosen = chosen | (picks == places_t[col : col + 1, :])
        out = jnp.dot(
            chosen.astype(jnp.bfloat16), first[...], preferred_element_type=jnp.float32
        )
        pack(group, out, send)

        post(group, send, arrived, send_sem, recv_sem, 1)
        return carry

    lax.fori_loop(0, GROUPS, load_group, 0)
    arrived[0] = send[0]

    for load in loads[6:9]:
        load.wait()
    tokens = first[...]
    gated = jnp.dot(tokens, sgate[...], preferred_element_type=jnp.float32)
    lifted = jnp.dot(tokens, sup[...], preferred_element_type=jnp.float32)
    inner = (gated / (1.0 + jnp.exp(-gated)) * lifted).astype(jnp.bfloat16)
    total[...] = ALPHA * tokens.astype(jnp.float32) + jnp.dot(
        inner, sdown[...], preferred_element_type=jnp.float32
    )
    for load in loads[9:12]:
        load.wait()

    def expert_group(group, carry):
        wait_blocks(group, arrived, recv_sem)
        unpack(group, arrived)
        tokens = rows[...]
        gated = jnp.dot(tokens, gate[...], preferred_element_type=jnp.float32)
        lifted = jnp.dot(tokens, up[...], preferred_element_type=jnp.float32)
        inner = (gated / (1.0 + jnp.exp(-gated)) * lifted).astype(jnp.bfloat16)
        out = jnp.dot(inner, down[...], preferred_element_type=jnp.float32)
        pack(group, out, made)
        post(group, made, returned, back_sem, ret_sem, -1)
        return carry

    lax.fori_loop(0, GROUPS, expert_group, 0)
    returned[0] = made[0]

    def combine_group(group, carry):
        wait_blocks(group, returned, ret_sem)
        unpack(group, returned)
        picks = iota((128, GROUP_ROWS), 1) + group * GROUP_ROWS
        share = jnp.zeros((128, GROUP_ROWS), jnp.float32)
        for col in range(TOP_K):
            share = share + jnp.where(
                picks == places[:, col : col + 1], gates[:, col : col + 1], 0.0
            )
        high = share.astype(jnp.bfloat16)
        low = (share - high.astype(jnp.float32)).astype(jnp.bfloat16)
        tokens = rows[...]
        total[...] += jnp.dot(high, tokens, preferred_element_type=jnp.float32) + jnp.dot(
            low, tokens, preferred_element_type=jnp.float32
        )
        return carry

    lax.fori_loop(0, GROUPS, combine_group, 0)
    out_ref[...] = layer_norm(total[...], gain2_ref[...], bias2_ref[...]).astype(jnp.bfloat16)
    sent = send.at[pl.ds(0, 127)]
    pltpu.make_async_copy(sent, sent, send_sem).wait()
    pltpu.make_async_copy(sent, sent, back_sem).wait()
    pltpu.make_async_copy(fifteen, fifteen, msg_sem).wait()
    pltpu.make_async_copy(arrivals, arrivals, head_sem).wait()


def per_device(
    hidden_in, queries, key_value_latent, keys_rope, latent_norm_gain, latent_up_weight,
    attn_gain, out_proj, norm1_gain, norm1_bias, expert_ids, route_weights,
    gate_proj, up_proj, down_proj, shared_gate, shared_up, shared_down, norm2_gain, norm2_bias,
):
    bf16, f32 = jnp.bfloat16, jnp.float32
    vmem = pl.BlockSpec(memory_space=pltpu.VMEM)
    hbm = pl.BlockSpec(memory_space=pltpu.HBM)
    blocks = pltpu.VMEM((GROUPS * PER_GROUP, SLOTS * TILES, 128), bf16)
    tables = jnp.asarray(rotation_tables(16, 128))
    layer = pl.pallas_call(
        layer_kernel,
        out_shape=jax.ShapeDtypeStruct((128, D), bf16),
        in_specs=[hbm] * 21,
        out_specs=vmem,
        scratch_shapes=[
            pltpu.VMEM((TOP_K, 128), jnp.int32),
            pltpu.VMEM((TOP_K, 128), f32),
            pltpu.VMEM((QK_ROPE, 128), bf16),
            pltpu.VMEM((1, 512), f32),
            pltpu.VMEM((1, 1024), f32),
            pltpu.VMEM((1, D), f32),
            pltpu.VMEM((1, D), f32),
            pltpu.VMEM((1, D), f32),
            pltpu.VMEM((1, D), f32),
            pltpu.VMEM((128, 512), bf16),
            pltpu.VMEM((512, 2048), bf16),
            pltpu.VMEM((128, 1536), bf16),
            pltpu.VMEM((32, 128), f32),
            pltpu.VMEM((128, D), bf16),
            pltpu.VMEM((1024, D), bf16),
            pltpu.VMEM((D, 512), bf16),
            pltpu.VMEM((D, 512), bf16),
            pltpu.VMEM((512, D), bf16),
            pltpu.VMEM((D, 512), bf16),
            pltpu.VMEM((D, 512), bf16),
            pltpu.VMEM((512, D), bf16),
            pltpu.VMEM((1536, 128), bf16),
            pltpu.VMEM((16, 256, 128), bf16),
            pltpu.VMEM((16, 256, 128), bf16),
            pltpu.VMEM((2048, 192), bf16),
            pltpu.VMEM((192, 2048), bf16),
            pltpu.VMEM((64, 2048), bf16),
            pltpu.VMEM((2, 8, 256, 256), f32),
            pltpu.VMEM((36, 256, 256), bf16),
            pltpu.VMEM((16, 64, 128), bf16),
            pltpu.VMEM((16, 64, 128), bf16),
            pltpu.VMEM((128, D), bf16),
            pltpu.VMEM((TOP_K, 128), jnp.int32),
            pltpu.VMEM((128, TOP_K), jnp.int32),
            pltpu.VMEM((128, TOP_K), f32),
            blocks, blocks, blocks, blocks,
            pltpu.VMEM((GROUP_ROWS * TILES, 128), f32),
            pltpu.VMEM((GROUP_ROWS, D), bf16),
            pltpu.VMEM((128, D), f32),
            pltpu.SemaphoreType.DMA((21,)),
            pltpu.SemaphoreType.DMA,
            pltpu.SemaphoreType.DMA,
            pltpu.SemaphoreType.DMA,
            pltpu.SemaphoreType.DMA,
            pltpu.SemaphoreType.DMA,
            pltpu.SemaphoreType.DMA,
            pltpu.SemaphoreType.DMA((GROUPS,)),
            pltpu.SemaphoreType.DMA,
            pltpu.SemaphoreType.DMA((GROUPS,)),
        ],
        compiler_params=pltpu.CompilerParams(
            collective_id=1, has_side_effects=True, vmem_limit_bytes=52 * 2**20
        ),
    )
    operands = (
        expert_ids[0].T, route_weights[0].T, keys_rope[0].T, latent_norm_gain[None],
        attn_gain[None], norm1_gain[None], norm1_bias[None], norm2_gain[None], norm2_bias[None],
        key_value_latent[0], latent_up_weight, queries[0], tables, hidden_in[0],
        out_proj, gate_proj, up_proj, down_proj, shared_gate, shared_up, shared_down,
    )
    result = layer(*(pltpu.with_memory_space_constraint(a, pltpu.HBM) for a in operands))
    return result[None]


def solution(mesh):
    in_specs = (
        P("dp", "sp", None),
        P("dp", "sp", None),
        P("dp", "sp", None),
        P("dp", "sp", None),
        P(),
        P(),
        P(),
        P(),
        P(),
        P(),
        P("dp", "sp", None),
        P("dp", "sp", None),
        P(("sp", "dp"), None, None),
        P(("sp", "dp"), None, None),
        P(("sp", "dp"), None, None),
        P(),
        P(),
        P(),
        P(),
        P(),
    )
    out_specs = P("dp", "sp", None)
    return jax.shard_map(
        per_device, mesh=mesh, in_specs=in_specs, out_specs=out_specs, check_vma=False
    )
```

```python
import math

import jax
import jax.numpy as jnp
import numpy as np
from jax import lax
from jax.experimental import pallas as pl
from jax.experimental.pallas import tpu as pltpu
from jax.sharding import PartitionSpec as P

D = 2048
ATTENTION_HEADS = 16
PLAIN_HEAD_WIDTH = 64
QK_ROPE = 32
VALUE_HEAD_WIDTH = 64
TOP_K = 4


ALPHA = 2.0**0.25
ROUTED = 2.5
THETA = 10000.0


def rms_scaled(values, scaling):
    widened = values.astype(jnp.float32)
    return (
        widened * lax.rsqrt(jnp.mean(widened * widened, axis=-1, keepdims=True) + 1e-06) * scaling
    )


def layer_norm(values, scaling, bias_add):
    centre = values - jnp.mean(values, axis=-1, keepdims=True)
    spread = jnp.mean(centre * centre, axis=-1, keepdims=True)
    return centre * lax.rsqrt(spread + 1e-05) * scaling + bias_add


def rotation_tables(devices, rows):
    frequency = np.power(THETA, -np.arange(0, QK_ROPE, 2) / QK_ROPE).astype(np.float32)
    positions = np.arange(devices * rows, dtype=np.float32).reshape(devices, 1, rows)
    angles = (positions * frequency[None, :, None]).astype(np.float64)
    return np.concatenate([np.cos(angles), np.sin(angles)], axis=1).astype(np.float32)


MESH = pl.DeviceIdType.MESH
GROUPS = 8
PER_GROUP = 16
SLOTS = 6
GROUP_ROWS = PER_GROUP * SLOTS
TILES = D // 128


def position_of(sp, dp):
    return sp // 4, sp % 4, dp // 2, dp % 2


def order_of(expert_ids, here):
    z, y, x, c = here
    ez, ey, ex, ec = expert_ids // 32, (expert_ids // 8) % 4, (expert_ids // 2) % 4, expert_ids % 2
    dz, dy, dx, dc = (ez - z) & 3, (ey - y) & 3, (ex - x) & 3, (ec + c) & 1
    return (((dz + dy + dx) & 3) * 2 + dc) * 16 + dy * 4 + dx


def iota(shape, dim):
    return lax.broadcasted_iota(jnp.int32, shape, dim)


def layer_kernel(
    ids_t_hbm, weights_t_hbm, rope_t_hbm, latent_gain_hbm, attn_gain_hbm,
    gain1_hbm, bias1_hbm, gain2_hbm, bias2_hbm,
    latent_hbm, latent_up_hbm, queries_hbm, tables_hbm, hidden_hbm,
    out_proj_hbm, gate_hbm, up_hbm, down_hbm, sgate_hbm, sup_hbm, sdown_hbm,
    out_ref,
    ids_t_ref, weights_t_ref, rope_t_ref, latent_gain_ref, attn_gain_ref,
    gain1_ref, bias1_ref, gain2_ref, bias2_ref,
    latent, latent_up, queries, tables, hidden,
    out_proj, gate, up, down, sgate, sup, sdown,
    turned, message, letters, keys, asked, values_t, scores, probs, heads_out, heads_in,
    first, places_t, places, gates, send, arrived, made, returned, flat, rows, total,
    load_sem, msg_sem, letter_sem, value_sem, head_sem, heads_sem,
    send_sem, recv_sem, back_sem, ret_sem, all_sem,
):
    sp, dp = lax.axis_index("sp"), lax.axis_index("dp")
    here = position_of(sp, dp)
    loads = [
        pltpu.make_async_copy(src, dst, load_sem.at[i])
        for i, (src, dst) in enumerate(
            (
                (latent_hbm, latent), (latent_up_hbm, latent_up), (queries_hbm, queries),
                (tables_hbm.at[sp], tables), (hidden_hbm, hidden), (out_proj_hbm, out_proj),
                (sgate_hbm, sgate), (sup_hbm, sup), (sdown_hbm, sdown),
                (gate_hbm.at[0], gate), (up_hbm.at[0], up), (down_hbm.at[0], down),
                (latent_gain_hbm, latent_gain_ref), (rope_t_hbm, rope_t_ref),
                (ids_t_hbm, ids_t_ref), (weights_t_hbm, weights_t_ref),
                (attn_gain_hbm, attn_gain_ref), (gain1_hbm, gain1_ref), (bias1_hbm, bias1_ref),
                (gain2_hbm, gain2_ref), (bias2_hbm, bias2_ref),
            )
        )
    ]
    for i in (3, 13, 2, 0, 12, 1):
        loads[i].start()
    barrier = pltpu.get_barrier_semaphore()

    columns = [lax.rem(dp + j, 8) for j in range(8)]

    def greet(i, carry):
        peer = (lax.rem(sp + i, 16), dp)
        pl.semaphore_signal(barrier, inc=1, device_id=peer, device_id_type=MESH)
        return carry

    lax.fori_loop(1, 16, greet, 0)
    for j in range(1, 8):
        pl.semaphore_signal(barrier, inc=1, device_id=(sp, columns[j]), device_id_type=MESH)
    z, y, x, c = here
    z_plus, y_plus, x_plus = ([lax.rem(v + j, 4) for j in range(4)] for v in (z, y, x))
    y_minus, x_minus = ([lax.rem(v + 4 - j, 4) for j in range(4)] for v in (y, x))

    loads[3].wait()
    loads[13].wait()
    cosine, sine = tables[0:16, :], tables[16:32, :]

    def turn(both):
        a, b = both[0:16].astype(jnp.float32), both[16:32].astype(jnp.float32)
        return jnp.concatenate([a * cosine - b * sine, b * cosine + a * sine], axis=0).astype(
            jnp.bfloat16
        )

    rope_t = turn(rope_t_ref[...])
    loads[2].wait()
    for tile in range(12):
        turned[tile * 128 : tile * 128 + 128, :] = queries[:, tile * 128 : tile * 128 + 128].T
    for head in range(16):
        block = turned[head * 96 : head * 96 + 96, :]
        message[head, 0:64, :] = block[0:64]
        message[head, 64:96, :] = turn(block[64:96])
        message[head, 96:128, :] = rope_t
    loads[0].wait()
    loads[12].wait()
    normed = rms_scaled(latent[...], latent_gain_ref[...]).astype(jnp.bfloat16)
    loads[1].wait()
    keys_values = jnp.dot(normed, latent_up[...], preferred_element_type=jnp.float32).astype(
        jnp.bfloat16
    )
    for head in range(16):
        message[head, 128:256, :] = keys_values[:, head * 128 : head * 128 + 128].T
    pl.semaphore_wait(barrier, 22)

    def deliver(rows, sem):
        for k in range(1, 16):
            peer = z_plus[(k // 4 - k) % 4] * 4 + y_plus[k % 4]
            pltpu.make_async_remote_copy(
                message.at[peer, rows], letters.at[sp, rows], msg_sem, sem,
                device_id=(peer, dp), device_id_type=MESH,
            ).start()

    keys_part, values_part = pl.ds(0, 192), pl.ds(192, 64)
    deliver(keys_part, letter_sem)
    deliver(values_part, value_sem)
    for j in range(1, 8):
        pl.semaphore_signal(all_sem, inc=1, device_id=(sp, columns[j]), device_id_type=MESH)
    letters[sp] = message[sp]
    for i in (14, 15, 4, 5, 16, 17, 18, 6, 7, 8, 9, 10, 11, 19, 20):
        loads[i].start()

    loads[14].wait()
    loads[15].wait()
    ids_t = ids_t_ref[...]
    named_t = jnp.zeros((128, 128), jnp.bool_)
    for col in range(TOP_K):
        named_t = named_t | (iota((128, 128), 0) == ids_t[col : col + 1, :])
    before = (iota((128, 128), 0) < iota((128, 128), 1)).astype(jnp.bfloat16)
    count_t = jnp.dot(named_t.astype(jnp.bfloat16), before, preferred_element_type=jnp.float32)
    order_t = order_of(ids_t, here)
    for col in range(TOP_K):
        slot = jnp.sum(
            jnp.where(iota((128, 128), 0) == ids_t[col : col + 1, :], count_t, 0.0),
            axis=0, keepdims=True,
        )
        places_t[col : col + 1, :] = order_t[col : col + 1, :] * SLOTS + slot.astype(jnp.int32)
    def upright(short):
        filler = jnp.zeros((128 - TOP_K, 128), short.dtype)
        return jnp.concatenate([short, filler], axis=0).T[:, 0:TOP_K]

    places[...] = upright(places_t[...].astype(jnp.float32)).astype(jnp.int32)
    weights = weights_t_ref[...]
    gates[...] = upright(weights / jnp.sum(weights, axis=0, keepdims=True) * ROUTED)

    asked[...] = jnp.zeros_like(asked)
    fifteen = message.at[pl.ds(0, 15)]
    some = message.at[pl.ds(0, 15), keys_part]
    pltpu.make_async_copy(some, some, letter_sem).wait()
    for block in range(16):
        span = slice(block * 128, block * 128 + 128)
        top, plain = letters[block, 0:128, :], letters[block, 128:192, :]
        keys[span, 0:128] = top.T
        keys[span, 128:192] = plain.T
        asked[96:128, span] = top[64:96]
        asked[128:192, span] = top[0:64]

    factor = math.log2(math.e) / math.sqrt(PLAIN_HEAD_WIDTH + QK_ROPE)

    def place_of(index, other):
        return index * (index + 1) // 2 + other

    def weigh(index):
        asking = asked[:, index * 256 : index * 256 + 256]
        peak, weight = None, 0.0
        for other in range(index + 1):
            part = jnp.dot(
                keys[other * 256 : other * 256 + 256, :], asking,
                preferred_element_type=jnp.float32,
            )
            if other == index:
                part = jnp.where(iota((256, 256), 0) <= iota((256, 256), 1), part, -jnp.inf)
            scores[index % 2, other] = part
            high = jnp.max(part, axis=0, keepdims=True)
            peak = high if peak is None else jnp.maximum(peak, high)
        peak = peak * factor
        for other in range(index + 1):
            part = jnp.exp2(scores[index % 2, other] * factor - peak)
            weight = weight + jnp.sum(part, axis=0, keepdims=True)
            probs[place_of(index, other)] = part.astype(jnp.bfloat16)
        return weight

    def attend(index, weight):
        mixed = 0.0
        for other in range(index + 1):
            mixed = mixed + jnp.dot(
                values_t[:, other * 256 : other * 256 + 256], probs[place_of(index, other)],
                preferred_element_type=jnp.float32,
            )
        mixed = (mixed / weight).astype(jnp.bfloat16)
        heads_out[2 * index] = mixed[:, 0:128]
        heads_out[2 * index + 1] = mixed[:, 128:256]

    def give_back(base, count):
        def give(k, carry):
            peer = base + (sp + k) % count

            @pl.when(peer != sp)
            def _():
                pltpu.make_async_remote_copy(
                    heads_out.at[peer], heads_in.at[sp], head_sem, heads_sem,
                    device_id=(peer, dp), device_id_type=MESH,
                ).start()

            return carry

        lax.fori_loop(0, count, give, 0)

    sums = [weigh(index) for index in range(8)]
    some = message.at[pl.ds(0, 15), values_part]
    pltpu.make_async_copy(some, some, value_sem).wait()
    for block in range(16):
        values_t[:, block * 128 : block * 128 + 128] = letters[block, 192:256, :]
    for index in range(8):
        attend(index, sums[index])
        if index in (3, 5, 7):
            give_back(*{3: (0, 8), 5: (8, 4), 7: (12, 4)}[index])
    heads_in[sp] = heads_out[sp]
    for load in loads[4:6] + loads[16:21]:
        load.wait()
    arrivals = heads_out.at[pl.ds(0, 15)]
    pltpu.make_async_copy(arrivals, arrivals, heads_sem).wait()
    attended = heads_in[...].reshape(1024, 128).T
    attn_normed = rms_scaled(attended, attn_gain_ref[...]).astype(jnp.bfloat16)
    mixed = jnp.dot(attn_normed, out_proj[...], preferred_element_type=jnp.float32)
    first[...] = layer_norm(
        ALPHA * hidden[...].astype(jnp.float32) + mixed, gain1_ref[...], bias1_ref[...]
    ).astype(jnp.bfloat16)

    def pack(group, source, target):
        for tile in range(TILES):
            flat[pl.ds(tile, GROUP_ROWS, stride=TILES), :] = source[:, tile * 128 : tile * 128 + 128]
        target[pl.ds(group * PER_GROUP, PER_GROUP)] = (
            flat[...].astype(jnp.bfloat16).reshape(PER_GROUP, SLOTS * TILES, 128)
        )

    def unpack(group, source):
        flat[...] = (
            source[pl.ds(group * PER_GROUP, PER_GROUP)]
            .reshape(GROUP_ROWS * TILES, 128)
            .astype(jnp.float32)
        )
        for tile in range(TILES):
            rows[:, tile * 128 : tile * 128 + 128] = flat[
                pl.ds(tile, GROUP_ROWS, stride=TILES), :
            ].astype(jnp.bfloat16)

    def post(group, source, target, out_sem, in_sem, sign):
        turn_z, core = z + 8 + sign * (group // 2), lax.rem(c + group % 2, 2)
        z_of = [lax.rem(turn_z - sign * j, 4) for j in range(4)]
        y_of, x_of = (y_plus, x_plus) if sign > 0 else (y_minus, x_minus)
        for i in (0, 5, 10, 15, 1, 6, 11, 12, 2, 7, 8, 13, 3, 4, 9, 14):
            dy, dx = i // 4, i % 4

            def start(i=i, dy=dy, dx=dx):
                k = group * PER_GROUP + i
                peer = (z_of[(dy + dx) % 4] * 4 + y_of[dy], x_of[dx] * 2 + core)
                pltpu.make_async_remote_copy(
                    source.at[k], target.at[k], out_sem, in_sem.at[group],
                    device_id=peer, device_id_type=MESH,
                ).start()

            if i == 0:
                pl.when(group > 0)(start)
            else:
                start()

    def wait_blocks(group, buffer, sem):
        @pl.when(group == 0)
        def _():
            block = buffer.at[pl.ds(0, PER_GROUP - 1)]
            pltpu.make_async_copy(block, block, sem.at[group]).wait()

        @pl.when(group > 0)
        def _():
            block = buffer.at[pl.ds(0, PER_GROUP)]
            pltpu.make_async_copy(block, block, sem.at[group]).wait()

    pl.semaphore_wait(all_sem, 7)

    def load_group(group, carry):
        picks = iota((GROUP_ROWS, 128), 0) + group * GROUP_ROWS
        chosen = jnp.zeros((GROUP_ROWS, 128), jnp.bool_)
        for col in range(TOP_K):
            chosen = chosen | (picks == places_t[col : col + 1, :])
        out = jnp.dot(
            chosen.astype(jnp.bfloat16), first[...], preferred_element_type=jnp.float32
        )
        pack(group, out, send)

        post(group, send, arrived, send_sem, recv_sem, 1)
        return carry

    lax.fori_loop(0, GROUPS, load_group, 0)
    arrived[0] = send[0]

    for load in loads[6:9]:
        load.wait()
    tokens = first[...]
    gated = jnp.dot(tokens, sgate[...], preferred_element_type=jnp.float32)
    lifted = jnp.dot(tokens, sup[...], preferred_element_type=jnp.float32)
    inner = (gated / (1.0 + jnp.exp(-gated)) * lifted).astype(jnp.bfloat16)
    total[...] = ALPHA * tokens.astype(jnp.float32) + jnp.dot(
        inner, sdown[...], preferred_element_type=jnp.float32
    )
    for load in loads[9:12]:
        load.wait()

    def expert_group(group, carry):
        wait_blocks(group, arrived, recv_sem)
        unpack(group, arrived)
        tokens = rows[...]
        gated = jnp.dot(tokens, gate[...], preferred_element_type=jnp.float32)
        lifted = jnp.dot(tokens, up[...], preferred_element_type=jnp.float32)
        inner = (gated / (1.0 + jnp.exp(-gated)) * lifted).astype(jnp.bfloat16)
        out = jnp.dot(inner, down[...], preferred_element_type=jnp.float32)
        pack(group, out, made)
        post(group, made, returned, back_sem, ret_sem, -1)
        return carry

    lax.fori_loop(0, GROUPS, expert_group, 0)
    returned[0] = made[0]

    def combine_group(group, carry):
        wait_blocks(group, returned, ret_sem)
        unpack(group, returned)
        picks = iota((128, GROUP_ROWS), 1) + group * GROUP_ROWS
        share = jnp.zeros((128, GROUP_ROWS), jnp.float32)
        for col in range(TOP_K):
            share = share + jnp.where(
                picks == places[:, col : col + 1], gates[:, col : col + 1], 0.0
            )
        high = share.astype(jnp.bfloat16)
        low = (share - high.astype(jnp.float32)).astype(jnp.bfloat16)
        tokens = rows[...]
        total[...] += jnp.dot(high, tokens, preferred_element_type=jnp.float32) + jnp.dot(
            low, tokens, preferred_element_type=jnp.float32
        )
        return carry

    lax.fori_loop(0, GROUPS, combine_group, 0)
    out_ref[...] = layer_norm(total[...], gain2_ref[...], bias2_ref[...]).astype(jnp.bfloat16)
    sent = send.at[pl.ds(0, 127)]
    pltpu.make_async_copy(sent, sent, send_sem).wait()
    pltpu.make_async_copy(sent, sent, back_sem).wait()
    pltpu.make_async_copy(fifteen, fifteen, msg_sem).wait()
    pltpu.make_async_copy(arrivals, arrivals, head_sem).wait()


def per_device(
    hidden_in, queries, key_value_latent, keys_rope, latent_norm_gain, latent_up_weight,
    attn_gain, out_proj, norm1_gain, norm1_bias, expert_ids, route_weights,
    gate_proj, up_proj, down_proj, shared_gate, shared_up, shared_down, norm2_gain, norm2_bias,
):
    bf16, f32 = jnp.bfloat16, jnp.float32
    vmem = pl.BlockSpec(memory_space=pltpu.VMEM)
    hbm = pl.BlockSpec(memory_space=pltpu.HBM)
    blocks = pltpu.VMEM((GROUPS * PER_GROUP, SLOTS * TILES, 128), bf16)
    tables = jnp.asarray(rotation_tables(16, 128))
    layer = pl.pallas_call(
        layer_kernel,
        out_shape=jax.ShapeDtypeStruct((128, D), bf16),
        in_specs=[hbm] * 21,
        out_specs=vmem,
        scratch_shapes=[
            pltpu.VMEM((TOP_K, 128), jnp.int32),
            pltpu.VMEM((TOP_K, 128), f32),
            pltpu.VMEM((QK_ROPE, 128), bf16),
            pltpu.VMEM((1, 512), f32),
            pltpu.VMEM((1, 1024), f32),
            pltpu.VMEM((1, D), f32),
            pltpu.VMEM((1, D), f32),
            pltpu.VMEM((1, D), f32),
            pltpu.VMEM((1, D), f32),
            pltpu.VMEM((128, 512), bf16),
            pltpu.VMEM((512, 2048), bf16),
            pltpu.VMEM((128, 1536), bf16),
            pltpu.VMEM((32, 128), f32),
            pltpu.VMEM((128, D), bf16),
            pltpu.VMEM((1024, D), bf16),
            pltpu.VMEM((D, 512), bf16),
            pltpu.VMEM((D, 512), bf16),
            pltpu.VMEM((512, D), bf16),
            pltpu.VMEM((D, 512), bf16),
            pltpu.VMEM((D, 512), bf16),
            pltpu.VMEM((512, D), bf16),
            pltpu.VMEM((1536, 128), bf16),
            pltpu.VMEM((16, 256, 128), bf16),
            pltpu.VMEM((16, 256, 128), bf16),
            pltpu.VMEM((2048, 192), bf16),
            pltpu.VMEM((192, 2048), bf16),
            pltpu.VMEM((64, 2048), bf16),
            pltpu.VMEM((2, 8, 256, 256), f32),
            pltpu.VMEM((36, 256, 256), bf16),
            pltpu.VMEM((16, 64, 128), bf16),
            pltpu.VMEM((16, 64, 128), bf16),
            pltpu.VMEM((128, D), bf16),
            pltpu.VMEM((TOP_K, 128), jnp.int32),
            pltpu.VMEM((128, TOP_K), jnp.int32),
            pltpu.VMEM((128, TOP_K), f32),
            blocks, blocks, blocks, blocks,
            pltpu.VMEM((GROUP_ROWS * TILES, 128), f32),
            pltpu.VMEM((GROUP_ROWS, D), bf16),
            pltpu.VMEM((128, D), f32),
            pltpu.SemaphoreType.DMA((21,)),
            pltpu.SemaphoreType.DMA,
            pltpu.SemaphoreType.DMA,
            pltpu.SemaphoreType.DMA,
            pltpu.SemaphoreType.DMA,
            pltpu.SemaphoreType.DMA,
            pltpu.SemaphoreType.DMA,
            pltpu.SemaphoreType.DMA((GROUPS,)),
            pltpu.SemaphoreType.DMA,
            pltpu.SemaphoreType.DMA((GROUPS,)),
            pltpu.SemaphoreType.REGULAR,
        ],
        compiler_params=pltpu.CompilerParams(
            collective_id=1, has_side_effects=True, vmem_limit_bytes=52 * 2**20
        ),
    )
    operands = (
        expert_ids[0].T, route_weights[0].T, keys_rope[0].T, latent_norm_gain[None],
        attn_gain[None], norm1_gain[None], norm1_bias[None], norm2_gain[None], norm2_bias[None],
        key_value_latent[0], latent_up_weight, queries[0], tables, hidden_in[0],
        out_proj, gate_proj, up_proj, down_proj, shared_gate, shared_up, shared_down,
    )
    result = layer(*(pltpu.with_memory_space_constraint(a, pltpu.HBM) for a in operands))
    return result[None]


def solution(mesh):
    in_specs = (
        P("dp", "sp", None),
        P("dp", "sp", None),
        P("dp", "sp", None),
        P("dp", "sp", None),
        P(),
        P(),
        P(),
        P(),
        P(),
        P(),
        P("dp", "sp", None),
        P("dp", "sp", None),
        P(("sp", "dp"), None, None),
        P(("sp", "dp"), None, None),
        P(("sp", "dp"), None, None),
        P(),
        P(),
        P(),
        P(),
        P(),
    )
    out_specs = P("dp", "sp", None)
    return jax.shard_map(
        per_device, mesh=mesh, in_specs=in_specs, out_specs=out_specs, check_vma=False
    )
```
